32 devices in a mesh: sp: 8 (over z, y), tp: 4 (over x, core).
Axes of the slice: x: 2, y: 2, z: 4, core: 2. Of those that a mesh axis runs over, the one named last changes fastest.
Arguments:
- query_one: bfloat16 [2048, 512], P('sp', 'tp'), may hold values from -190 to 190
- query_two: bfloat16 [2048, 512], P('sp', 'tp'), may hold values from -190 to 190
- key_one: bfloat16 [2048, 512], P('sp', 'tp'), may hold values from -10 to 10
- key_two: bfloat16 [2048, 512], P('sp', 'tp'), may hold values from -10 to 10
- values: bfloat16 [2048, 1024], P('sp', 'tp'), may hold values from -6 to 6
- mix_lambda: float32 [8], P('tp'), may hold values from 0.3 to 0.8
- head_gain: float32 [128], replicated, may hold values from 0.1 to 1.9
- stream: bfloat16 [2048, 2048], P('sp', 'tp'), may hold values from -6 to 6
- out_weight: bfloat16 [1024, 2048], P('tp'), may hold values from -0.1875 to 0.1875
- first_gain: float32 [2048], replicated, may hold values from 0.1 to 1.9
- up_weight: bfloat16 [2048, 4096], P('sp', 'tp'), may hold values from -0.125 to 0.125
- down_weight: bfloat16 [4096, 2048], P('tp', 'sp'), may hold values from -0.09375 to 0.09375
- second_gain: float32 [2048], replicated, may hold values from 0.1 to 1.9
Outputs:
- layer_out: bfloat16 [2048, 2048], P(('sp', 'tp'))
The draws below stay inside these ranges and needn't reach their ends.
All inputs are finite; a program needn't handle non-finite values.
Results may differ from the reference program's by a relative error of at most 0.019.
Values may be sent and summed in bfloat16 or wider, within the bound.
A program may use at most 128 MiB of HBM per device.

```python
import math
import jax
import jax.numpy as jnp
from jax import lax

D = 2048
HEADS = 8
QK = 64
VD = 128
FF = 4096
SEQ = 2048
HV = 1024


def drawn_pair(key, which):
    key_query = jax.random.fold_in(key, 11 + which)
    key_keys = jax.random.fold_in(key, 23 + which)
    width = HEADS * QK
    keys_drawn = jnp.clip(jax.random.normal(key_keys, (SEQ, width), jnp.float32), -7.0, 7.0) * 1.3
    queries = jnp.clip(jax.random.normal(key_query, (SEQ, width), jnp.float32), -7.0, 7.0) * 1.3
    return (queries, keys_drawn)


def draw_query_one(key, part):
    return drawn_pair(key, 1)[0].astype(jnp.bfloat16)


def draw_key_one(key, part):
    return drawn_pair(key, 1)[1].astype(jnp.bfloat16)


def draw_query_two(key, part):
    return drawn_pair(key, 2)[0].astype(jnp.bfloat16)


def draw_key_two(key, part):
    return drawn_pair(key, 2)[1].astype(jnp.bfloat16)


def block_scale(rng, dims, split, low, high):
    level, own = 1.0, jax.random.fold_in(rng, 6)
    for dim, blocks in split:
        heights = jnp.exp(jax.random.uniform(jax.random.fold_in(own, dim), (blocks,), jnp.float32, low / len(split), high / len(split)))
        level = level * jnp.repeat(heights, dims[dim] // blocks).reshape([-1 if axis == dim else 1 for axis in range(len(dims))])
    return level


def noise(stream_key, shape, scale, reach, cuts=(), held_as=jnp.bfloat16):
    result = scale * jax.random.normal(stream_key, shape, jnp.float32)
    if cuts:
        result = result * block_scale(stream_key, shape, cuts, -0.22, 0.18)
    return jnp.clip(result, -reach, reach).astype(held_as)


def setup_inputs(seed: int = 0) -> dict:
    key_of = jax.random.split(jax.random.key(seed), 14)
    query_one = draw_query_one(jax.random.fold_in(key_of[13], 71), 0)
    query_two = draw_query_two(jax.random.fold_in(key_of[13], 71), 0)
    key_one = draw_key_one(jax.random.fold_in(key_of[13], 71), 0)
    key_two = draw_key_two(jax.random.fold_in(key_of[13], 71), 0)
    values = noise(key_of[4], (SEQ, HV), 1.0, 6.0, ((0, 8), (1, 4)))
    mix_lambda = jnp.clip(0.3 + 0.5 * jax.random.uniform(key_of[5], (HEADS,), jnp.float32) ** block_scale(key_of[5], (HEADS,), ((0, 4),), -0.2, 0.2), 0.3, 0.8)
    head_gain = jnp.clip(1.0 + 0.18 * jax.random.normal(key_of[6], (VD,), jnp.float32), 0.1, 1.9)
    stream = noise(key_of[7], (SEQ, D), 1.0, 6.0, ((0, 8), (1, 4)))
    out_weight = noise(key_of[8], (HV, D), HV ** -0.5, 0.1875, ((0, 4),))
    first_gain = jnp.clip(1.0 + 0.18 * jax.random.normal(key_of[9], (D,), jnp.float32), 0.1, 1.9)
    up_weight = noise(key_of[10], (D, FF), D ** -0.5, 0.125, ((0, 8), (1, 4)))
    down_weight = noise(key_of[11], (FF, D), FF ** -0.5, 0.09375, ((0, 4), (1, 8)))
    second_gain = jnp.clip(1.0 + 0.18 * jax.random.normal(key_of[12], (D,), jnp.float32), 0.1, 1.9)
    return dict(query_one=query_one, query_two=query_two, key_one=key_one, key_two=key_two, values=values, mix_lambda=mix_lambda, head_gain=head_gain, stream=stream, out_weight=out_weight, first_gain=first_gain, up_weight=up_weight, down_weight=down_weight, second_gain=second_gain)


alpha_mix = 2.0 ** 0.5

def layer_norm(value, gain):
    centre = lax.optimization_barrier(jnp.mean(value, axis=-1, keepdims=True))
    spread = lax.optimization_barrier(jnp.mean(jnp.square(value - centre), axis=-1, keepdims=True))
    return (value - centre) * lax.rsqrt(spread + 1e-05) * gain

def one_map(query_blk, keys, values):
    scores = jnp.dot(query_blk, keys.T, preferred_element_type=jnp.float32) * QK ** (-0.5)
    shifted = scores - lax.optimization_barrier(jnp.max(scores, axis=-1, keepdims=True))
    expo = jnp.exp(shifted)
    total = lax.optimization_barrier(jnp.sum(expo, axis=-1, keepdims=True))
    return jnp.dot(expo.astype(jnp.bfloat16), values, preferred_element_type=jnp.float32) / total

def reference(query_one, query_two, key_one, key_two, values, mix_lambda, head_gain, stream, out_weight, first_gain, up_weight, down_weight, second_gain):

    def heads(array, width):
        return jnp.transpose(array.reshape(SEQ, HEADS, width), (1, 0, 2))
    qblk = math.gcd(SEQ, 512)
    nblk = SEQ // qblk

    def per_head(args):
        q_one, q_two, k_one, k_two, vals, weight = args
        q_one = q_one.reshape(nblk, qblk, QK)
        q_two = q_two.reshape(nblk, qblk, QK)

        def per_block(pair):
            return one_map(pair[0], k_one, vals) - weight * one_map(pair[1], k_two, vals)
        return lax.map(per_block, (q_one, q_two)).reshape(SEQ, VD)
    mixed = lax.map(per_head, (heads(query_one, QK), heads(query_two, QK), heads(key_one, QK), heads(key_two, QK), heads(values, VD), mix_lambda))
    normed = mixed * lax.rsqrt(lax.optimization_barrier(jnp.mean(jnp.square(mixed), axis=-1, keepdims=True)) + 1e-05) * head_gain * 0.8
    attended = jnp.transpose(normed.astype(jnp.bfloat16), (1, 0, 2)).reshape(SEQ, HV)
    pre = alpha_mix * stream.astype(jnp.float32) + jnp.dot(attended, out_weight, preferred_element_type=jnp.float32)
    hidden_in = layer_norm(pre, first_gain).astype(jnp.bfloat16)
    upper = jnp.dot(hidden_in, up_weight, preferred_element_type=jnp.float32)
    act = jnp.square(jax.nn.relu(upper)).astype(jnp.bfloat16)
    post = alpha_mix * hidden_in.astype(jnp.float32) + jnp.dot(act, down_weight, preferred_element_type=jnp.float32)
    return layer_norm(post, second_gain).astype(jnp.bfloat16)
```

```python
import functools

import jax
import jax.numpy as jnp
from jax import lax
from jax.experimental import pallas as pl
from jax.experimental.pallas import tpu as pltpu
from jax.sharding import PartitionSpec as P

MESH = pl.DeviceIdType.MESH
F32, BF16 = jnp.float32, jnp.bfloat16
ALPHA = 2.0**0.5
NT = (((1,), (1,)), ((), ()))
TN = (((0,), (0,)), ((), ()))
DIRS = (1, -1)


def layer_norm(value, gain):
    centre = jnp.mean(value, axis=-1, keepdims=True)
    spread = jnp.mean(jnp.square(value - centre), axis=-1, keepdims=True)
    return (value - centre) * lax.rsqrt(spread + 1e-05) * gain


def kernel(
    nsp, ntp, heads,
    lam_ref, q1_ref, q2_ref, k1_ref, k2_ref, v_ref, hg_ref, st_ref, ow_ref, g1_ref, up_ref, dn_ref, g2_ref,
    out_ref,
    lam_all, qin, kin, qsl, slab, hg, g1, g2,
    q_buf, qm, m_run, l_run, acc, kv_buf, up_buf, dn_buf, ow_buf, st_buf, at_snd, at_buf,
    pre, h_own, h_buf, act, sib_snd, sib_buf, part, own_part, red_snd, red_buf,
    loc_sem, lms, gqs, gks, kvr, upr, dnr, upy, dny, owx, ows, sts, ats, hps, hss, sbs, rds,
):
    s, t = lax.axis_index("sp"), lax.axis_index("tp")
    nz, nth = nsp // 2, ntp // 2
    hops = nz // 2
    ng = 2 * nth
    z, y = s // 2, s % 2
    x, c = t // 2, t % 2
    sib_t = x * 2 + (1 - c)
    y_sp = z * 2 + (1 - y)
    grp = y * nth + x
    tok = q1_ref.shape[0]
    share = tok // ntp
    fh = up_ref.shape[1] // 2
    vd = acc.shape[1]
    qw = q_buf.shape[2]
    qk = qw // 2
    d = pre.shape[1]
    out_w = dn_buf.shape[2]
    head_t = x * 2 + y

    def rc(src, dst, sems, i, sp, tp, arrive=None):
        arrive = i if arrive is None else arrive
        return pltpu.make_async_remote_copy(
            src_ref=src, dst_ref=dst, send_sem=sems.at[0, i], recv_sem=sems.at[1, arrive],
            device_id={"sp": sp, "tp": tp}, device_id_type=MESH,
        )

    def each(lo, hi, body):
        if hi - lo <= 4:
            for k in range(lo, hi):
                body(k)
        else:
            lax.fori_loop(lo, hi, lambda k, carry: (body(k), carry)[1], 0)

    def zat(off):
        return lax.rem(z + 2 * nz + off, nz)

    def lc(src, dst, i):
        return pltpu.make_async_copy(src, dst, loc_sem.at[i])

    def up_half(j):
        return up_ref.at[:, pl.ds(pl.multiple_of(j * fh, fh), fh)]

    def dn_half(j):
        return dn_ref.at[pl.ds(pl.multiple_of(j * fh, fh), fh), :]

    def rows_of(tt):
        return pl.ds(pl.multiple_of(tt * share, share), share)

    qk_loads = [
        lc(q1_ref, qin.at[0], 0),
        lc(q2_ref, qin.at[1], 1),
        lc(k1_ref, kin.at[0], 2),
        lc(k2_ref, kin.at[1], 3),
    ]
    v_loads = [
        lc(v_ref.at[:, pl.ds(j * vd, vd)], slab.at[j, :, pl.ds(qw, vd)], 4 + j) for j in range(heads)
    ]
    n0 = 4 + heads
    gain_loads = [lc(hg_ref, hg, n0), lc(g1_ref, g1, n0 + 1), lc(g2_ref, g2, n0 + 2)]
    up_load = lc(up_half(y), up_buf.at[s], n0 + 3)
    dn_load = lc(dn_half(y), dn_buf.at[s], n0 + 4)
    ow_load = lc(ow_ref, ow_buf.at[t], n0 + 5)
    st_load = lc(st_ref.at[rows_of(t), :], st_buf.at[t], n0 + 6)
    for ld in qk_loads + v_loads:
        ld.start()

    def half_of(dr):
        return 0 if dr > 0 else 1

    def piece(buf, origin, side, hf):
        r2 = buf.shape[1] // 2
        return buf.at[origin * 2 + lax.rem(y + side, 2), pl.ds(hf * r2, r2)]

    def slot(dr, k, side, hf):
        return (half_of(dr) * hops + (k - 1)) * 4 + side * 2 + hf

    def ring(item, dr, k, side, hf):
        buf, sems = item
        ref = piece(buf, zat(-dr * (k - 1)), side, hf)
        return rc(ref, ref, sems, slot(dr, k, side, hf), zat(dr) * 2 + y, t)

    def ring_in(item, dr, k, side, hf):
        buf, sems = item
        ref = piece(buf, zat(-dr * k), side, hf)
        return rc(ref, ref, sems, slot(dr, k, side, hf), zat(dr) * 2 + y, t)

    def halves(dr, last=False):
        first = half_of(dr)
        return (first,) if last else (first, 1 - first)

    def ring_first(item, side):
        for n in range(2):
            for dr in DIRS:
                ring(item, dr, 1, side, halves(dr)[n]).start()

    def relay(item, dr, k, side):
        hf = half_of(dr)
        ring_in(item, dr, k, side, hf).wait_recv()
        ring(item, dr, k + 1, side, hf).start()
        if hops > 2:
            @pl.when(k < hops - 1)
            def _():
                ring_in(item, dr, k, side, 1 - hf).wait_recv()
                ring(item, dr, k + 1, side, 1 - hf).start()

    def rest(item, dr, k, side):
        hf = 1 - half_of(dr)
        if hops > 2:
            pl.when(k == hops - 1)(lambda: ring_in(item, dr, k, side, hf).wait_recv())
        else:
            ring_in(item, dr, k, side, hf).wait_recv()

    def last_in(item, side):
        for dr in DIRS:
            ring_in(item, dr, hops, side, half_of(dr)).wait_recv()

    def relay_all(item, side):
        each(1, hops, lambda k: [relay(item, dr, k, side) for dr in DIRS])

    def ring_sent(item):
        def one(k):
            for dr in DIRS:
                for side in range(2):
                    for hf in range(2):
                        if hf == half_of(dr):
                            ring(item, dr, k, side, hf).wait_send()
                        else:
                            ring(item, dr, k, side, hf).wait_send()

        each(1, hops, one)
        for dr in DIRS:
            for side in range(2):
                ring(item, dr, hops, side, half_of(dr)).wait_send()

    kv_item, up_item, dn_item = (kv_buf, kvr), (up_buf, upr), (dn_buf, dnr)

    def lam_c():
        return rc(lam_all.at[c], lam_all.at[c], lms, 0, s, sib_t)

    def q_c(j):
        return rc(qsl.at[j], q_buf.at[y], gqs, j, z * 2 + c, x * 2 + j, y)

    def q_in(side):
        yy = lax.rem(y + side, 2)
        return rc(q_buf.at[yy], q_buf.at[yy], gqs, 0, y_sp, t, yy)

    def kv_c(j):
        return rc(slab.at[j], kv_buf.at[s], gks, j, z * 2 + c, x * 2 + j, y)

    def kv_in(side):
        yy = lax.rem(y + side, 2)
        ref = kv_buf.at[z * 2 + yy]
        return rc(ref, ref, gks, 0, y_sp, t, yy)

    def to_self(j):
        return (c == y) & (c == j)

    def up_y():
        return rc(up_half(1 - y), up_buf.at[s], upy, 0, y_sp, t)

    def dn_y():
        return rc(dn_half(1 - y), dn_buf.at[s], dny, 0, y_sp, t)

    def y_in(buf, sems):
        ref = buf.at[y_sp]
        return rc(ref, ref, sems, 0, y_sp, t)

    def ow_x(k):
        return rc(ow_ref, ow_buf.at[t], owx, k, s, lax.rem(x + k, nth) * 2 + c)

    def ow_s0():
        return rc(ow_ref, ow_buf.at[t], ows, 0, s, sib_t)

    def ow_s(k):
        b = lax.rem(x + nth - k, nth) * 2 + c
        return rc(ow_buf.at[b], ow_buf.at[b], ows, k, s, sib_t)

    def st_c(k):
        td = lax.rem(t + k, ntp)
        return rc(st_ref.at[rows_of(td), :], st_buf.at[t], sts, k, s, td)

    def at_cols():
        return pl.ds(pl.multiple_of(c * vd, vd), vd)

    def at_c(yy, tt):
        rows = pl.ds((yy * ntp + tt) * share, share)
        return rc(
            at_snd.at[rows, :], at_buf.at[head_t, :, at_cols()], ats, yy * ntp + tt,
            z * 2 + yy, tt, head_t * 2 + c,
        )

    def at_in(hd):
        ref = at_buf.at[hd // 2, :, pl.ds((hd % 2) * vd, vd)]
        return rc(ref, ref, ats, 0, y_sp, t, hd)

    def grp_dev(g):
        return z * 2 + g // nth, lax.rem(g, nth) * 2 + c

    def h_p(k):
        sp, tp = grp_dev(lax.rem(grp + k, ng))
        return rc(h_own, h_buf.at[c, grp], hps, k, sp, tp)

    def h_s0():
        return rc(h_own, h_buf.at[c, grp], hss, 0, s, sib_t)

    def h_s(k):
        g = lax.rem(grp + ng - k, ng)
        return rc(h_buf.at[c, g], h_buf.at[c, g], hss, k, s, sib_t)

    def sib_c(zz):
        return rc(sib_snd.at[zz], sib_buf.at[zz], sbs, zz, s, sib_t)

    def red_c(zz, k):
        g = lax.rem(grp + k, ng)
        sp, tp = grp_dev(g)
        return rc(red_snd.at[zz, g], red_buf.at[zz, grp], rds, zz * ng + k, sp, tp)

    barrier = pltpu.get_barrier_semaphore()

    def greet(sp, tp):
        pl.semaphore_signal(barrier, inc=1, device_id={"sp": sp, "tp": tp}, device_id_type=MESH)

    for k in range(1, 2 * ntp):
        o = lax.rem(y * ntp + t + k, 2 * ntp)
        greet(z * 2 + o // ntp, lax.rem(o, ntp))
    for dr in DIRS:
        greet(zat(dr) * 2 + y, t)

    for ld in qk_loads:
        ld.wait()
    for j in range(heads):
        at = slice(j * qk, (j + 1) * qk)
        qsl[j] = jnp.concatenate([qin[0, :, at], qin[1, :, at]], axis=1)
        slab[j, :, :qw] = jnp.concatenate([kin[0, :, at], kin[1, :, at]], axis=1)
        lam_all[c, j] = jnp.full(lam_all.shape[2:], lam_ref[0, j], F32)
    for ld in v_loads:
        ld.wait()
    pl.semaphore_wait(barrier, 2 * ntp - 1 + 2)

    for j in range(heads):
        pl.when(jnp.logical_not(to_self(j)))(lambda: q_c(j).start())
    for j in range(heads):
        pl.when(jnp.logical_not(to_self(j)))(lambda: kv_c(j).start())
    for j in range(heads):
        @pl.when(to_self(j))
        def _():
            q_buf[y] = qsl[j]
            kv_buf[s] = slab[j]

    lam_c().start()
    up_y().start()
    each(1, ntp, lambda k: st_c(k).start())
    each(1, nth, lambda k: ow_x(k).start())
    ow_s0().start()
    dn_y().start()
    for ld in gain_loads + [st_load, ow_load, up_load, dn_load]:
        ld.start()

    m_run[...] = jnp.full(m_run.shape, -1e30, F32)
    l_run[...] = jnp.zeros(l_run.shape, F32)
    acc[...] = jnp.zeros(acc.shape, F32)

    pl.when(c != y)(lambda: kv_in(0).wait_recv())
    ring_first(kv_item, 0)
    pl.when(c != y)(lambda: q_in(0).wait_recv())
    q_in(1).wait_recv()
    scale = qk ** (-0.5)
    lane = lax.broadcasted_iota(jnp.int32, (tok, qw), 1)
    for i in range(2):
        qv = q_buf[i].astype(F32) * scale
        for mp in range(2):
            keep = (lane >= mp * qk) & (lane < (mp + 1) * qk)
            qm[mp, i * tok : (i + 1) * tok, :] = jnp.where(keep, qv, 0.0).astype(BF16)

    def absorb(block):
        v = block[:, qw:]
        for r in range(2):
            sc = lax.dot_general(block[:, :qw], qm[r], NT, preferred_element_type=F32)
            old = m_run[r]
            new = jnp.maximum(old, jnp.max(sc, axis=0, keepdims=True))
            fac = jnp.exp(old - new)
            ex = jnp.exp(sc - new)
            l_run[r] = l_run[r] * fac + jnp.sum(ex, axis=0, keepdims=True)
            acc[r] = acc[r] * fac + lax.dot_general(
                v, ex.astype(BF16), TN, preferred_element_type=F32
            )
            m_run[r] = new

    def own_up(side):
        if side == 0:
            r2 = up_ref.shape[0] // 2
            for n in range(2):
                for dr in DIRS:
                    own_first(up_ref, up_item, dr, halves(dr)[n], r2).start()
        else:
            y_in(up_buf, upy).wait_recv()
            ring_first(up_item, 1)

    def own_first(ref, item, dr, hf, r2):
        buf, sems = item
        if ref is up_ref:
            src = up_ref.at[pl.ds(hf * r2, r2), pl.ds(pl.multiple_of(y * fh, fh), fh)]
        else:
            src = dn_ref.at[pl.ds(pl.multiple_of(y * fh + hf * r2, r2), r2), :]
        return rc(src, buf.at[s, pl.ds(hf * r2, r2)], sems, slot(dr, 1, 0, hf), zat(dr) * 2 + y, t)

    def own_dn(side):
        if side == 0:
            r2 = fh // 2
            for n in range(2):
                for dr in DIRS:
                    own_first(dn_ref, dn_item, dr, halves(dr)[n], r2).start()
        else:
            y_in(dn_buf, dny).wait_recv()
            ring_first(dn_item, 1)

    def step(i, carry):
        k = (i + 2) // 4
        r = lax.rem(i + 2, 4)
        mid = (k > 0) & (k < hops)

        @pl.when(i == 1)
        def _():
            pl.when(jnp.bool_(True))(lambda: kv_in(1).wait_recv())
            ring_first(kv_item, 1)

        for side in range(2):
            @pl.when(mid & (r == 2 * side))
            def _():
                for dr in DIRS:
                    relay(kv_item, dr, k, side)
                rest(kv_item, 1, k, side)

            @pl.when(mid & (r == 2 * side + 1))
            def _():
                rest(kv_item, -1, k, side)

            @pl.when((k == hops) & (r == side))
            def _():
                last_in(kv_item, side)

        @pl.when(i == 4 * hops - 4)
        def _():
            own_up(0)
            own_up(1)

        side = jnp.where(k == 0, r - 2, jnp.where(k == hops, r, r // 2))
        off = jnp.where(mid & (lax.rem(r, 2) == 1), k, -k)
        absorb(kv_buf.at[zat(off) * 2 + lax.rem(y + side, 2)])
        return carry

    lax.fori_loop(0, 2 * nz, step, 0)

    for ld in gain_loads:
        ld.wait()
    lam_c().wait_recv()
    lam = lam_all[y, c][:, :1]
    mixed = acc[0] / l_run[0] - lam * (acc[1] / l_run[1])
    inv = lax.rsqrt(jnp.mean(jnp.square(mixed), axis=0, keepdims=True) + 1e-05)
    normed = jnp.transpose(mixed * inv) * hg[...] * 0.8
    at_snd[...] = normed.astype(BF16)
    spots = [(yy, tt) for yy in range(2) for tt in range(ntp)]
    for yy, tt in spots:
        mine = (yy == y) & (tt == t)
        pl.when(jnp.logical_not(mine))(lambda: at_c(yy, tt).start())

        @pl.when(mine)
        def _():
            n = (yy * ntp + tt) * share
            at_buf[head_t, :, at_cols()] = at_snd[n : n + share, :]

    relay_all(up_item, 0)
    own_dn(0)
    relay_all(up_item, 1)
    own_dn(1)

    for k in range(1, nth):
        ow_x(k).wait_recv()
        ow_s(k).start()
    st_load.wait()
    each(1, ntp, lambda k: st_c(k).wait_recv())
    cols = st_ref.shape[1]
    for b in range(ntp):
        pre[:, b * cols : (b + 1) * cols] = ALPHA * st_buf[b].astype(F32)
    for hd in range(2 * ntp):
        pl.when(head_t * 2 + c != hd)(lambda: at_in(hd).wait_recv())
    ow_load.wait()
    ow_s0().wait_recv()
    for k in range(1, nth):
        ow_s(k).wait_recv()
    for b in range(ntp):
        at = slice(b * cols, (b + 1) * cols)
        tot = pre[:, at]
        for tt in range(ntp):
            tot += jnp.dot(at_buf[tt], ow_buf[tt, :, at], preferred_element_type=F32)
        pre[:, at] = tot
    h_own[...] = layer_norm(pre[...], g1[...]).astype(BF16)
    each(1, ng, lambda k: h_p(k).start())
    h_s0().start()
    h_buf[c, grp] = h_own[...]

    def h_fwd(k):
        h_p(k).wait_recv()
        h_s(k).start()

    each(1, ng, h_fwd)
    relay_all(dn_item, 0)
    up_load.wait()
    for side in range(2):
        each(1, hops, lambda k: [rest(up_item, dr, k, side) for dr in DIRS])
        last_in(up_item, side)
    h_s0().wait_recv()
    each(1, ng, lambda k: h_s(k).wait_recv())

    half = ng * share
    for side in range(2):
        parts = 2 if fh % 256 == 0 else 1
        for n in range(parts):
            wide = fh // parts
            at = slice(n * wide, (n + 1) * wide)
            hid = h_buf[side].reshape(half, d)
            w = up_buf[:, :, at].reshape(d, wide)
            up = jnp.dot(hid, w, preferred_element_type=F32)
            act[side, :, at] = jnp.square(jnp.maximum(up, 0.0)).astype(BF16)

    dn_load.wait()

    def unit(u):
        k = (u + 1) // 2
        return k, zat(jnp.where((lax.rem(u, 2) == 0) & (k < hops), k, -k))

    def finish(u):
        zz = unit(u)[1]
        sib_c(zz).wait_recv()
        for k in range(ng - 1, 0, -1):
            g = lax.rem(grp + k, ng)
            rows = pl.ds(pl.multiple_of(g * share, share), share)
            red_snd[zz, g] = (part[zz, :, rows, :] + sib_buf[zz, :, rows, :].astype(F32)).astype(BF16)
            red_c(zz, k).start()
        rows = pl.ds(pl.multiple_of(grp * share, share), share)
        own_part[zz] = part[zz, :, rows, :] + sib_buf[zz, :, rows, :].astype(F32)

    def down(u, carry):
        k, zz = unit(u)

        @pl.when(u == 1)
        def _():
            relay_all(dn_item, 1)

        @pl.when((k > 0) & (k < hops))
        def _():
            for dr in DIRS:
                @pl.when(lax.rem(u, 2) == (1 if dr > 0 else 0))
                def _():
                    for side in range(2):
                        rest(dn_item, dr, k, side)

        @pl.when(k == hops)
        def _():
            for side in range(2):
                last_in(dn_item, side)

        for yy in range(2):
            res = jnp.dot(act[1 - c], dn_buf[zz * 2 + yy], preferred_element_type=F32)
            sib_snd[zz, yy] = res.astype(BF16)
        sib_c(zz).start()
        for yy in range(2):
            part[zz, yy] = jnp.dot(act[c], dn_buf[zz * 2 + yy], preferred_element_type=F32)
        pl.when(u > 0)(lambda: finish(u - 1))
        return carry

    lax.fori_loop(0, nz, down, 0)
    finish(nz - 1)

    for zz in range(nz):
        for k in range(1, ng):
            red_c(zz, k).wait_recv()
        for yy in range(2):
            at = slice((zz * 2 + yy) * out_w, (zz * 2 + yy + 1) * out_w)
            tot = own_part[zz, yy] + ALPHA * h_own[:, at].astype(F32)
            for k in range(ng - 1, 0, -1):
                tot += red_buf[zz, lax.rem(grp + ng - k, ng), yy].astype(F32)
            pre[:, at] = tot
    out_ref[...] = layer_norm(pre[...], g2[...]).astype(BF16)

    for j in range(heads):
        @pl.when(jnp.logical_not(to_self(j)))
        def _():
            q_c(j).wait_send()
            kv_c(j).wait_send()

    for yy, tt in spots:
        mine = (yy == y) & (tt == t)
        pl.when(jnp.logical_not(mine))(lambda: at_c(yy, tt).wait_send())
    for item in (kv_item, up_item, dn_item):
        ring_sent(item)
    lam_c().wait_send()
    up_y().wait_send()
    dn_y().wait_send()
    ow_s0().wait_send()
    h_s0().wait_send()
    each(0, nz, lambda zz: [sib_c(zz).wait_send()] + [red_c(zz, k).wait_send() for k in range(1, ng)])
    for first, last, fns in ((1, nth, (ow_x, ow_s)), (1, ntp, (st_c,)), (1, ng, (h_p, h_s))):
        each(first, last, lambda k: [f(k).wait_send() for f in fns])


def local(nsp, ntp, q1, q2, k1, k2, vals, lam, hg, stream, ow, g1, up, dn, g2):
    tok = q1.shape[0]
    heads = lam.shape[0]
    hv = vals.shape[1]
    vd = hv // heads
    d = ow.shape[1]
    nz, nth = nsp // 2, ntp // 2
    ng = 2 * nth
    share = tok // ntp
    fh = up.shape[1] // 2
    qk = q1.shape[1] // heads
    half, out_w = ng * share, dn.shape[1]
    vm = pl.BlockSpec(memory_space=pltpu.VMEM)
    sm = pl.BlockSpec(memory_space=pltpu.SMEM)
    hbm = pl.BlockSpec(memory_space=pl.ANY)
    sem = lambda n: pltpu.SemaphoreType.DMA((2, n))
    return pl.pallas_call(
        functools.partial(kernel, nsp, ntp, heads),
        out_shape=jax.ShapeDtypeStruct((share, d), BF16),
        in_specs=[sm] + [hbm] * 12,
        out_specs=vm,
        scratch_shapes=[
            pltpu.VMEM((2, heads, 1, 128), F32),
            pltpu.VMEM((2, tok, heads * qk), BF16),
            pltpu.VMEM((2, tok, heads * qk), BF16),
            pltpu.VMEM((heads, tok, 2 * qk), BF16),
            pltpu.VMEM((heads, tok, 2 * qk + vd), BF16),
            pltpu.VMEM((1, vd), F32),
            pltpu.VMEM((1, d), F32),
            pltpu.VMEM((1, d), F32),
            pltpu.VMEM((2, tok, 2 * qk), BF16),
            pltpu.VMEM((2, 2 * tok, 2 * qk), BF16),
            pltpu.VMEM((2, 1, 2 * tok), F32),
            pltpu.VMEM((2, 1, 2 * tok), F32),
            pltpu.VMEM((2, vd, 2 * tok), F32),
            pltpu.VMEM((nsp, tok, 2 * qk + vd), BF16),
            pltpu.VMEM((nsp, up.shape[0], fh), BF16),
            pltpu.VMEM((nsp, fh, out_w), BF16),
            pltpu.VMEM((ntp,) + ow.shape, BF16),
            pltpu.VMEM((ntp, share, stream.shape[1]), BF16),
            pltpu.VMEM((2 * tok, vd), BF16),
            pltpu.VMEM((ntp, share, hv), BF16),
            pltpu.VMEM((share, d), F32),
            pltpu.VMEM((share, d), BF16),
            pltpu.VMEM((2, ng, share, d), BF16),
            pltpu.VMEM((2, half, fh), BF16),
            pltpu.VMEM((nz, 2, half, out_w), BF16),
            pltpu.VMEM((nz, 2, half, out_w), BF16),
            pltpu.VMEM((nz, 2, half, out_w), F32),
            pltpu.VMEM((nz, 2, share, out_w), F32),
            pltpu.VMEM((nz, ng, 2, share, out_w), BF16),
            pltpu.VMEM((nz, ng, 2, share, out_w), BF16),
            pltpu.SemaphoreType.DMA((4 + heads + 7,)),
            sem(1), sem(heads), sem(heads), sem(4 * nz), sem(4 * nz), sem(4 * nz), sem(1), sem(1),
            sem(nth), sem(nth), sem(ntp), sem(2 * ntp), sem(ng), sem(ng), sem(nz), sem(nz * ng),
        ],
        compiler_params=pltpu.CompilerParams(
            collective_id=0, has_side_effects=True, vmem_limit_bytes=60 * 1024 * 1024
        ),
    )(
        lam.reshape(1, heads), q1, q2, k1, k2, vals, hg.reshape(1, vd), stream, ow,
        g1.reshape(1, d), up, dn, g2.reshape(1, d),
    )


def solution(mesh):
    in_specs = (
        P("sp", "tp"),
        P("sp", "tp"),
        P("sp", "tp"),
        P("sp", "tp"),
        P("sp", "tp"),
        P("tp"),
        P(),
        P("sp", "tp"),
        P("tp", None),
        P(),
        P("sp", "tp"),
        P("tp", "sp"),
        P(),
    )
    body = functools.partial(local, mesh.shape["sp"], mesh.shape["tp"])
    return jax.shard_map(
        body, mesh=mesh, in_specs=in_specs, out_specs=P(("sp", "tp"), None), check_vma=False
    )
```

```python
import functools

import jax
import jax.numpy as jnp
from jax import lax
from jax.experimental import pallas as pl
from jax.experimental.pallas import tpu as pltpu
from jax.sharding import PartitionSpec as P

MESH = pl.DeviceIdType.MESH
F32, BF16 = jnp.float32, jnp.bfloat16
ALPHA = 2.0**0.5
NT = (((1,), (1,)), ((), ()))
TN = (((0,), (0,)), ((), ()))


def layer_norm(value, gain):
    centre = jnp.mean(value, axis=-1, keepdims=True)
    spread = jnp.mean(jnp.square(value - centre), axis=-1, keepdims=True)
    return (value - centre) * lax.rsqrt(spread + 1e-05) * gain


def kernel(
    nsp, ntp, heads, pieces,
    lam_ref, q1_ref, q2_ref, k1_ref, k2_ref, v_ref, hg_ref, st_ref, ow_ref, g1_ref, up_ref, dn_ref, g2_ref,
    out_ref,
    lam_all, qin, kin, qsl, slab, hg, g1, g2,
    q_buf, qm, m_run, l_run, acc, kv_buf, up_buf, dn_buf, ow_buf, st_buf, at_snd, at_buf,
    pre, h_own, h_buf, act, sib_snd, sib_buf, part, own_part, red_snd, red_buf,
    loc_sem, lms, gqs, kvd, kvs, upz, upy, dnz, dny, owx, ows, sts, ats, hps, hss, sbs, rds,
):
    s, t = lax.axis_index("sp"), lax.axis_index("tp")
    nz, nth = nsp // 2, ntp // 2
    npair = nz // 2
    ng = 2 * nth
    z, y = s // 2, s % 2
    zh, zl = z // 2, z % 2
    mate = zh * 2 + 1 - zl
    x, c = t // 2, t % 2
    sib_t = x * 2 + (1 - c)
    y_sp = z * 2 + (1 - y)
    grp = zl * nth + x
    tok = q1_ref.shape[0]
    share = tok // ntp
    fh = up_ref.shape[1] // 2
    vd = acc.shape[1]
    qw = q_buf.shape[2]
    qk = qw // 2
    d = pre.shape[1]
    out_w = dn_buf.shape[2]
    pw = out_w // pieces
    head_t = x * 2 + zl

    def rc(src, dst, sems, i, sp, tp, arrive=None):
        arrive = i if arrive is None else arrive
        return pltpu.make_async_remote_copy(
            src_ref=src, dst_ref=dst, send_sem=sems.at[0, i], recv_sem=sems.at[1, arrive],
            device_id={"sp": sp, "tp": tp}, device_id_type=MESH,
        )

    def each(lo, hi, body):
        if hi - lo <= 4:
            for k in range(lo, hi):
                body(k)
        else:
            lax.fori_loop(lo, hi, lambda k, carry: (body(k), carry)[1], 0)

    def lc(src, dst, i):
        return pltpu.make_async_copy(src, dst, loc_sem.at[i])

    def up_half(j):
        return up_ref.at[:, pl.ds(pl.multiple_of(j * fh, fh), fh)]

    def dn_rows(j):
        return pl.ds(pl.multiple_of(j * fh, fh), fh)

    def rows_of(tt):
        return pl.ds(pl.multiple_of(tt * share, share), share)

    qk_loads = [
        lc(q1_ref, qin.at[0], 0),
        lc(q2_ref, qin.at[1], 1),
        lc(k1_ref, kin.at[0], 2),
        lc(k2_ref, kin.at[1], 3),
    ]
    v_loads = [
        lc(v_ref.at[:, pl.ds(j * vd, vd)], slab.at[j, :, pl.ds(qw, vd)], 4 + j) for j in range(heads)
    ]
    n0 = 4 + heads
    gain_loads = [lc(hg_ref, hg, n0), lc(g1_ref, g1, n0 + 1), lc(g2_ref, g2, n0 + 2)]
    up_load = lc(up_half(zl), up_buf.at[s], n0 + 3)
    dn_load = lc(dn_ref.at[dn_rows(zl), :], dn_buf.at[s], n0 + 4)
    ow_load = lc(ow_ref, ow_buf.at[t], n0 + 5)
    st_load = lc(st_ref.at[rows_of(t), :], st_buf.at[t], n0 + 6)
    for ld in qk_loads + v_loads:
        ld.start()

    def lam_c():
        return rc(lam_all.at[c], lam_all.at[c], lms, 0, s, sib_t)

    def to_self(j):
        return (c == zl) & (y == c) & (j == y)

    self_worker = (c == zl) & (y == c)

    def q_c(j):
        return rc(qsl.at[j], q_buf.at[zl], gqs, j, (zh * 2 + c) * 2 + j, x * 2 + y, zl)

    def q_in(i):
        return rc(q_buf.at[i], q_buf.at[i], gqs, 0, y_sp, t, i)

    def kv_c(r, j):
        return rc(slab.at[j], kv_buf.at[s], kvd, r * heads + j, (r * 2 + c) * 2 + j, x * 2 + y, z)

    def kv_in(zz):
        ref = kv_buf.at[zz * 2 + c]
        return rc(ref, ref, kvd, 0, y_sp, t, zz)

    def kv_s(zz, side):
        ref = kv_buf.at[zz * 2 + side]
        return rc(ref, ref, kvs, zz, s, sib_t)

    def kv_out(fn, own):
        for j in range(heads):
            if own:
                pl.when(jnp.logical_not(to_self(j)))(lambda: fn(kv_c(zh, j)))
            else:
                each(1, npair, lambda q: fn(kv_c(lax.rem(zh + q, npair), j)))

    def up_z(zz):
        return rc(up_half(zz % 2), up_buf.at[s], upz, zz, zz * 2 + y, t, z)

    def up_zin(zz):
        ref = up_buf.at[zz * 2 + y]
        return rc(ref, ref, upz, 0, y_sp, t, zz)

    def up_y0():
        return rc(up_half(zl), up_buf.at[s], upy, z, y_sp, t)

    def up_y(zz, side=0):
        ref = up_buf.at[zz * 2 + lax.rem(y + side, 2)]
        return rc(ref, ref, upy, zz, y_sp, t)

    def cols_of(p):
        return pl.ds(p * pw, pw)

    def dn_z(zz, p):
        return rc(
            dn_ref.at[dn_rows(zz % 2), cols_of(p)], dn_buf.at[s, :, cols_of(p)],
            dnz, zz * pieces + p, zz * 2 + y, t, z * pieces + p,
        )

    def dn_zin(zz, p):
        ref = dn_buf.at[zz * 2 + y, :, cols_of(p)]
        return rc(ref, ref, dnz, 0, y_sp, t, zz * pieces + p)

    def dn_y0(p):
        return rc(
            dn_ref.at[dn_rows(zl), cols_of(p)], dn_buf.at[s, :, cols_of(p)], dny, z * pieces + p, y_sp, t
        )

    def dn_y(zz, p, side=0):
        ref = dn_buf.at[zz * 2 + lax.rem(y + side, 2), :, cols_of(p)]
        return rc(ref, ref, dny, zz * pieces + p, y_sp, t)

    def ow_x(k):
        return rc(ow_ref, ow_buf.at[t], owx, k, s, lax.rem(x + k, nth) * 2 + c)

    def ow_s0():
        return rc(ow_ref, ow_buf.at[t], ows, 0, s, sib_t)

    def ow_s(k):
        b = lax.rem(x + nth - k, nth) * 2 + c
        return rc(ow_buf.at[b], ow_buf.at[b], ows, k, s, sib_t)

    def st_c(k):
        td = lax.rem(t + k, ntp)
        return rc(st_ref.at[rows_of(td), :], st_buf.at[t], sts, k, s, td)

    def at_cols():
        return pl.ds(pl.multiple_of(y * vd, vd), vd)

    def at_c(i, tt):
        rows = pl.ds((i * ntp + tt) * share, share)
        return rc(
            at_snd.at[rows, :], at_buf.at[head_t, :, at_cols()], ats, i * ntp + tt,
            (zh * 2 + i) * 2 + c, tt, head_t * 2 + y,
        )

    def at_in(hd):
        ref = at_buf.at[hd // 2, :, pl.ds((hd % 2) * vd, vd)]
        return rc(ref, ref, ats, 0, y_sp, t, hd)

    def grp_dev(g):
        return (zh * 2 + g // nth) * 2 + y, lax.rem(g, nth) * 2 + c

    def h_p(k):
        sp, tp = grp_dev(lax.rem(grp + k, ng))
        return rc(h_own, h_buf.at[c, grp], hps, k, sp, tp)

    def h_s0():
        return rc(h_own, h_buf.at[c, grp], hss, 0, s, sib_t)

    def h_s(k):
        g = lax.rem(grp + ng - k, ng)
        return rc(h_buf.at[c, g], h_buf.at[c, g], hss, k, s, sib_t)

    def sib_c(n):
        return rc(sib_snd.at[n], sib_buf.at[n], sbs, n, s, sib_t)

    def red_c(n, k):
        g = lax.rem(grp + k, ng)
        sp, tp = grp_dev(g)
        return rc(red_snd.at[n, g], red_buf.at[n, grp], rds, n * ng + k, sp, tp)

    def other(q, m):
        r = lax.rem(zh + q, npair)
        return r * 2 + jnp.where(r > zh, m, 1 - m)

    def shared(zz):
        return (zz > z) == (mate > z)

    def others(fn):
        for m in range(2):
            each(1, npair, lambda q: fn(other(q, m)))

    barrier = pltpu.get_barrier_semaphore()

    def greet(sp, tp):
        pl.semaphore_signal(barrier, inc=1, device_id={"sp": sp, "tp": tp}, device_id_type=MESH)

    for o in range(4 * ntp):
        sp, tt = zh * 4 + o // ntp, o % ntp
        pl.when((sp != s) | (tt != t))(functools.partial(greet, sp, tt))

    def greet_far(q):
        for o in range(8):
            greet(lax.rem(zh + q, npair) * 4 + o // 2, x * 2 + o % 2)

    each(1, npair, greet_far)

    for ld in qk_loads:
        ld.wait()
    for j in range(heads):
        at = slice(j * qk, (j + 1) * qk)
        qsl[j] = jnp.concatenate([qin[0, :, at], qin[1, :, at]], axis=1)
        slab[j, :, :qw] = jnp.concatenate([kin[0, :, at], kin[1, :, at]], axis=1)
        lam_all[c, j] = jnp.full(lam_all.shape[2:], lam_ref[0, j], F32)
    for ld in v_loads:
        ld.wait()
    pl.semaphore_wait(barrier, 4 * ntp - 1 + 8 * (npair - 1))

    kv_out(lambda cp: cp.start(), False)
    for j in range(heads):
        pl.when(jnp.logical_not(to_self(j)))(lambda: q_c(j).start())
    kv_out(lambda cp: cp.start(), True)
    for j in range(heads):
        @pl.when(to_self(j))
        def _():
            q_buf[zl] = qsl[j]
            kv_buf[s] = slab[j]

    lam_c().start()
    each(1, ntp, lambda k: st_c(k).start())
    each(1, nth, lambda k: ow_x(k).start())
    ow_s0().start()
    others(lambda zz: up_z(zz).start())
    up_z(mate).start()
    up_y0().start()
    for ld in gain_loads + [st_load, ow_load, up_load, dn_load]:
        ld.start()

    def dn_far(early):
        for p in range(pieces):
            others(lambda zz: pl.when(shared(zz) != early)(lambda: dn_z(zz, p).start()))

    dn_far(True)

    m_run[...] = jnp.full(m_run.shape, -1e30, F32)
    l_run[...] = jnp.zeros(l_run.shape, F32)
    acc[...] = jnp.zeros(acc.shape, F32)
    scale = qk ** (-0.5)
    lane = lax.broadcasted_iota(jnp.int32, (tok, qw), 1)
    for i in range(2):
        pl.when(jnp.logical_not(self_worker & (zl == i)))(lambda: q_in(i).wait_recv())
        qv = q_buf[i].astype(F32) * scale
        for mp in range(2):
            keep = (lane >= mp * qk) & (lane < (mp + 1) * qk)
            qm[mp, i * tok : (i + 1) * tok, :] = jnp.where(keep, qv, 0.0).astype(BF16)

    def absorb(block):
        v = block[:, qw:]
        for r in range(2):
            sc = lax.dot_general(block[:, :qw], qm[r], NT, preferred_element_type=F32)
            old = m_run[r]
            new = jnp.maximum(old, jnp.max(sc, axis=0, keepdims=True))
            fac = jnp.exp(old - new)
            ex = jnp.exp(sc - new)
            l_run[r] = l_run[r] * fac + jnp.sum(ex, axis=0, keepdims=True)
            acc[r] = acc[r] * fac + lax.dot_general(
                v, ex.astype(BF16), TN, preferred_element_type=F32
            )
            m_run[r] = new

    def step(i, carry):
        zz = lax.rem(zh * 2 + i // 2, nz)
        own = lax.rem(i, 2) == 0

        @pl.when(own)
        def _():
            pl.when(jnp.logical_not(self_worker & (zz == z)))(lambda: kv_in(zz).wait_recv())
            kv_s(zz, c).start()

        pl.when(jnp.logical_not(own))(lambda: kv_s(zz, 1 - c).wait_recv())
        absorb(kv_buf.at[zz * 2 + jnp.where(own, c, 1 - c)])
        return carry

    lax.fori_loop(0, nsp, step, 0)

    for ld in gain_loads:
        ld.wait()
    lam_c().wait_recv()
    lam = lam_all[zl, y][:, :1]
    mixed = acc[0] / l_run[0] - lam * (acc[1] / l_run[1])
    inv = lax.rsqrt(jnp.mean(jnp.square(mixed), axis=0, keepdims=True) + 1e-05)
    normed = jnp.transpose(mixed * inv) * hg[...] * 0.8
    at_snd[...] = normed.astype(BF16)
    spots = [(i, tt) for i in range(2) for tt in range(ntp)]

    def at_mine(i, tt):
        return (i == zl) & (y == c) & (tt == t)

    for i, tt in spots:
        pl.when(jnp.logical_not(at_mine(i, tt)))(lambda: at_c(i, tt).start())

        @pl.when(at_mine(i, tt))
        def _():
            n = (i * ntp + tt) * share
            at_buf[head_t, :, at_cols()] = at_snd[n : n + share, :]

    def up_fwd(zz):
        up_zin(zz).wait_recv()
        up_y(zz).start()

    up_fwd(mate)
    for k in range(1, nth):
        ow_x(k).wait_recv()
        ow_s(k).start()
    st_load.wait()
    each(1, ntp, lambda k: st_c(k).wait_recv())
    cols = st_ref.shape[1]
    for b in range(ntp):
        pre[:, b * cols : (b + 1) * cols] = ALPHA * st_buf[b].astype(F32)
    for hd in range(2 * ntp):
        pl.when((y != c) | (head_t * 2 + y != hd))(lambda: at_in(hd).wait_recv())
    ow_load.wait()
    ow_s0().wait_recv()
    for k in range(1, nth):
        ow_s(k).wait_recv()
    for b in range(ntp):
        at = slice(b * cols, (b + 1) * cols)
        tot = pre[:, at]
        for tt in range(ntp):
            tot += jnp.dot(at_buf[tt], ow_buf[tt, :, at], preferred_element_type=F32)
        pre[:, at] = tot
    h_own[...] = layer_norm(pre[...], g1[...]).astype(BF16)
    each(1, ng, lambda k: h_p(k).start())
    h_s0().start()
    dn_far(False)
    for p in range(pieces):
        dn_z(mate, p).start()
    for p in range(pieces):
        dn_y0(p).start()
    h_buf[c, grp] = h_own[...]
    others(up_fwd)

    def h_fwd(k):
        h_p(k).wait_recv()
        h_s(k).start()

    each(1, ng, h_fwd)
    up_load.wait()
    each(0, nz, lambda zz: up_y(zz, 1).wait_recv())
    h_s0().wait_recv()
    each(1, ng, lambda k: h_s(k).wait_recv())

    half = ng * share
    for side in range(2):
        parts = 2 if fh % 256 == 0 else 1
        for n in range(parts):
            wide = fh // parts
            at = slice(n * wide, (n + 1) * wide)
            hid = h_buf[side].reshape(half, d)
            w = up_buf[:, :, at].reshape(d, wide)
            up = jnp.dot(hid, w, preferred_element_type=F32)
            act[side, :, at] = jnp.square(jnp.maximum(up, 0.0)).astype(BF16)

    dn_load.wait()

    def unit(u):
        w = u // pieces
        return jnp.where(w == 0, z, jnp.where(w == 1, mate, other(w // 2, lax.rem(w, 2))))

    def finish(n):
        sib_c(n).wait_recv()
        for k in range(ng - 1, 0, -1):
            g = lax.rem(grp + k, ng)
            rows = pl.ds(pl.multiple_of(g * share, share), share)
            red_snd[n, g] = (part[n, :, rows, :] + sib_buf[n, :, rows, :].astype(F32)).astype(BF16)
            red_c(n, k).start()
        rows = pl.ds(pl.multiple_of(grp * share, share), share)
        own_part[n] = part[n, :, rows, :] + sib_buf[n, :, rows, :].astype(F32)

    def down(w, carry):
        zz = unit(w * pieces)
        before = unit(w * pieces - pieces)
        for p in range(pieces):
            n = zz * pieces + p

            @pl.when(w > 0)
            def _():
                dn_zin(zz, p).wait_recv()
                dn_y(zz, p).start()

            dn_y(zz, p, 1).wait_recv()
            at = slice(p * pw, (p + 1) * pw)
            for yy in range(2):
                res = jnp.dot(act[1 - c], dn_buf[zz * 2 + yy, :, at], preferred_element_type=F32)
                sib_snd[n, yy] = res.astype(BF16)
            sib_c(n).start()
            for yy in range(2):
                part[n, yy] = jnp.dot(act[c], dn_buf[zz * 2 + yy, :, at], preferred_element_type=F32)
            if p > 0:
                finish(n - 1)
            else:
                pl.when(w > 0)(lambda: finish(before * pieces + pieces - 1))
        return carry

    lax.fori_loop(0, nz, down, 0)
    finish(unit(nz * pieces - pieces) * pieces + pieces - 1)

    for zz in range(nz):
        for p in range(pieces):
            n = zz * pieces + p
            for k in range(1, ng):
                red_c(n, k).wait_recv()
            for yy in range(2):
                lo = (zz * 2 + yy) * out_w + p * pw
                at = slice(lo, lo + pw)
                tot = own_part[n, yy] + ALPHA * h_own[:, at].astype(F32)
                for k in range(ng - 1, 0, -1):
                    tot += red_buf[n, lax.rem(grp + ng - k, ng), yy].astype(F32)
                pre[:, at] = tot
    out_ref[...] = layer_norm(pre[...], g2[...]).astype(BF16)

    for j in range(heads):
        pl.when(jnp.logical_not(to_self(j)))(lambda: q_c(j).wait_send())
    kv_out(lambda cp: cp.wait_send(), False)
    kv_out(lambda cp: cp.wait_send(), True)
    for i, tt in spots:
        pl.when(jnp.logical_not(at_mine(i, tt)))(lambda: at_c(i, tt).wait_send())

    def sent(zz):
        up_z(zz).wait_send()
        up_y(zz).wait_send()
        for p in range(pieces):
            dn_z(zz, p).wait_send()
            dn_y(zz, p).wait_send()

    others(sent)
    sent(mate)
    up_y0().wait_send()
    for p in range(pieces):
        dn_y0(p).wait_send()
    each(0, nz, lambda zz: kv_s(zz, c).wait_send())
    lam_c().wait_send()
    ow_s0().wait_send()
    h_s0().wait_send()
    each(0, nz * pieces, lambda n: [sib_c(n).wait_send()] + [red_c(n, k).wait_send() for k in range(1, ng)])
    for first, last, fns in ((1, nth, (ow_x, ow_s)), (1, ntp, (st_c,)), (1, ng, (h_p, h_s))):
        each(first, last, lambda k: [f(k).wait_send() for f in fns])


def local(nsp, ntp, q1, q2, k1, k2, vals, lam, hg, stream, ow, g1, up, dn, g2):
    tok = q1.shape[0]
    heads = lam.shape[0]
    hv = vals.shape[1]
    vd = hv // heads
    d = ow.shape[1]
    nz, nth = nsp // 2, ntp // 2
    ng = 2 * nth
    share = tok // ntp
    fh = up.shape[1] // 2
    qk = q1.shape[1] // heads
    half, out_w = ng * share, dn.shape[1]
    pieces = 2 if out_w % 256 == 0 else 1
    units, pw = nz * pieces, out_w // pieces
    vm = pl.BlockSpec(memory_space=pltpu.VMEM)
    sm = pl.BlockSpec(memory_space=pltpu.SMEM)
    hbm = pl.BlockSpec(memory_space=pl.ANY)
    sem = lambda n: pltpu.SemaphoreType.DMA((2, n))
    return pl.pallas_call(
        functools.partial(kernel, nsp, ntp, heads, pieces),
        out_shape=jax.ShapeDtypeStruct((share, d), BF16),
        in_specs=[sm] + [hbm] * 12,
        out_specs=vm,
        scratch_shapes=[
            pltpu.VMEM((2, heads, 1, 128), F32),
            pltpu.VMEM((2, tok, heads * qk), BF16),
            pltpu.VMEM((2, tok, heads * qk), BF16),
            pltpu.VMEM((heads, tok, 2 * qk), BF16),
            pltpu.VMEM((heads, tok, 2 * qk + vd), BF16),
            pltpu.VMEM((1, vd), F32),
            pltpu.VMEM((1, d), F32),
            pltpu.VMEM((1, d), F32),
            pltpu.VMEM((2, tok, 2 * qk), BF16),
            pltpu.VMEM((2, 2 * tok, 2 * qk), BF16),
            pltpu.VMEM((2, 1, 2 * tok), F32),
            pltpu.VMEM((2, 1, 2 * tok), F32),
            pltpu.VMEM((2, vd, 2 * tok), F32),
            pltpu.VMEM((nsp, tok, 2 * qk + vd), BF16),
            pltpu.VMEM((nsp, up.shape[0], fh), BF16),
            pltpu.VMEM((nsp, fh, out_w), BF16),
            pltpu.VMEM((ntp,) + ow.shape, BF16),
            pltpu.VMEM((ntp, share, stream.shape[1]), BF16),
            pltpu.VMEM((2 * tok, vd), BF16),
            pltpu.VMEM((ntp, share, hv), BF16),
            pltpu.VMEM((share, d), F32),
            pltpu.VMEM((share, d), BF16),
            pltpu.VMEM((2, ng, share, d), BF16),
            pltpu.VMEM((2, half, fh), BF16),
            pltpu.VMEM((units, 2, half, pw), BF16),
            pltpu.VMEM((units, 2, half, pw), BF16),
            pltpu.VMEM((units, 2, half, pw), F32),
            pltpu.VMEM((units, 2, share, pw), F32),
            pltpu.VMEM((units, ng, 2, share, pw), BF16),
            pltpu.VMEM((units, ng, 2, share, pw), BF16),
            pltpu.SemaphoreType.DMA((4 + heads + 7,)),
            sem(1), sem(max(heads, 2)), sem(max(nz // 2 * heads, nz)), sem(nz),
            sem(nz), sem(nz), sem(units), sem(units),
            sem(nth), sem(nth), sem(ntp), sem(2 * ntp), sem(ng), sem(ng), sem(units), sem(units * ng),
        ],
        compiler_params=pltpu.CompilerParams(
            collective_id=0, has_side_effects=True, vmem_limit_bytes=60 * 1024 * 1024
        ),
    )(
        lam.reshape(1, heads), q1, q2, k1, k2, vals, hg.reshape(1, vd), stream, ow,
        g1.reshape(1, d), up, dn, g2.reshape(1, d),
    )


def solution(mesh):
    in_specs = (
        P("sp", "tp"),
        P("sp", "tp"),
        P("sp", "tp"),
        P("sp", "tp"),
        P("sp", "tp"),
        P("tp"),
        P(),
        P("sp", "tp"),
        P("tp", None),
        P(),
        P("sp", "tp"),
        P("tp", "sp"),
        P(),
    )
    body = functools.partial(local, mesh.shape["sp"], mesh.shape["tp"])
    return jax.shard_map(
        body, mesh=mesh, in_specs=in_specs, out_specs=P(("sp", "tp"), None), check_vma=False
    )
```

```python
import functools

import jax
import jax.numpy as jnp
from jax import lax
from jax.experimental import pallas as pl
from jax.experimental.pallas import tpu as pltpu
from jax.sharding import PartitionSpec as P

MESH = pl.DeviceIdType.MESH
F32, BF16 = jnp.float32, jnp.bfloat16
ALPHA = 2.0**0.5
NT = (((1,), (1,)), ((), ()))
TN = (((0,), (0,)), ((), ()))


def layer_norm(value, gain):
    centre = jnp.mean(value, axis=-1, keepdims=True)
    spread = jnp.mean(jnp.square(value - centre), axis=-1, keepdims=True)
    return (value - centre) * lax.rsqrt(spread + 1e-05) * gain


def kernel(
    nsp, ntp, heads, pieces,
    lam_ref, q1_ref, q2_ref, k1_ref, k2_ref, v_ref, hg_ref, st_ref, ow_ref, g1_ref, up_ref, dn_ref, g2_ref,
    out_ref,
    lam_all, qin, kin, qsl, slab, hg, g1, g2,
    q_buf, qm, m_run, l_run, acc, kv_buf, up_buf, dn_buf, ow_buf, st_buf, at_snd, at_buf,
    pre, h_own, h_buf, act, sib_snd, sib_buf, part, own_part, red_snd, red_buf,
    loc_sem, lms, gqs, kvd, kvs, upz, upy, dnz, dny, owx, ows, sts, ats, hps, hss, sbs, rds,
):
    s, t = lax.axis_index("sp"), lax.axis_index("tp")
    nz, nth = nsp // 2, ntp // 2
    npair = nz // 2
    ng = 2 * nth
    z, y = s // 2, s % 2
    zh, zl = z // 2, z % 2
    mate = zh * 2 + 1 - zl
    x, c = t // 2, t % 2
    sib_t = x * 2 + (1 - c)
    y_sp = z * 2 + (1 - y)
    grp = zl * nth + x
    tok = q1_ref.shape[0]
    share = tok // ntp
    fh = up_ref.shape[1] // 2
    vd = acc.shape[1]
    qw = q_buf.shape[2]
    qk = qw // 2
    d = pre.shape[1]
    out_w = dn_buf.shape[2]
    pw = out_w // pieces
    head_t = x * 2 + zl

    def rc(src, dst, sems, i, sp, tp, arrive=None):
        arrive = i if arrive is None else arrive
        return pltpu.make_async_remote_copy(
            src_ref=src, dst_ref=dst, send_sem=sems.at[0, i], recv_sem=sems.at[1, arrive],
            device_id={"sp": sp, "tp": tp}, device_id_type=MESH,
        )

    def each(lo, hi, body):
        if hi - lo <= 4:
            for k in range(lo, hi):
                body(k)
        else:
            lax.fori_loop(lo, hi, lambda k, carry: (body(k), carry)[1], 0)

    def lc(src, dst, i):
        return pltpu.make_async_copy(src, dst, loc_sem.at[i])

    def up_half(j):
        return up_ref.at[:, pl.ds(pl.multiple_of(j * fh, fh), fh)]

    def dn_rows(j):
        return pl.ds(pl.multiple_of(j * fh, fh), fh)

    def rows_of(tt):
        return pl.ds(pl.multiple_of(tt * share, share), share)

    qk_loads = [
        lc(q1_ref, qin.at[0], 0),
        lc(q2_ref, qin.at[1], 1),
        lc(k1_ref, kin.at[0], 2),
        lc(k2_ref, kin.at[1], 3),
    ]
    v_loads = [
        lc(v_ref.at[:, pl.ds(j * vd, vd)], slab.at[j, :, pl.ds(qw, vd)], 4 + j) for j in range(heads)
    ]
    n0 = 4 + heads
    gain_loads = [lc(hg_ref, hg, n0), lc(g1_ref, g1, n0 + 1), lc(g2_ref, g2, n0 + 2)]
    up_load = lc(up_half(zl), up_buf.at[s], n0 + 3)
    dn_load = lc(dn_ref.at[dn_rows(zl), :], dn_buf.at[s], n0 + 4)
    ow_load = lc(ow_ref, ow_buf.at[t], n0 + 5)
    st_load = lc(st_ref.at[rows_of(t), :], st_buf.at[t], n0 + 6)
    for ld in qk_loads + v_loads:
        ld.start()

    def lam_c():
        return rc(lam_all.at[c], lam_all.at[c], lms, 0, s, sib_t)

    def to_self(j):
        return (c == zl) & (y == c) & (j == y)

    self_worker = (c == zl) & (y == c)

    def q_c(j):
        return rc(qsl.at[j], q_buf.at[zl], gqs, j, (zh * 2 + c) * 2 + j, x * 2 + y, zl)

    def q_in(i):
        return rc(q_buf.at[i], q_buf.at[i], gqs, 0, y_sp, t, i)

    def kv_c(r, j):
        return rc(slab.at[j], kv_buf.at[s], kvd, r * heads + j, (r * 2 + c) * 2 + j, x * 2 + y, z)

    def kv_in(zz):
        ref = kv_buf.at[zz * 2 + c]
        return rc(ref, ref, kvd, 0, y_sp, t, zz)

    def kv_s(zz, side):
        ref = kv_buf.at[zz * 2 + side]
        return rc(ref, ref, kvs, zz, s, sib_t)

    def kv_out(fn, own):
        for j in range(heads):
            if own:
                pl.when(jnp.logical_not(to_self(j)))(lambda: fn(kv_c(zh, j)))
            else:
                each(1, npair, lambda q: fn(kv_c(lax.rem(zh + q, npair), j)))

    def up_z(zz):
        return rc(up_half(zz % 2), up_buf.at[s], upz, zz, zz * 2 + y, t, z)

    def up_zin(zz):
        ref = up_buf.at[zz * 2 + y]
        return rc(ref, ref, upz, 0, y_sp, t, zz)

    def up_y0():
        return rc(up_half(zl), up_buf.at[s], upy, z, y_sp, t)

    def up_y(zz, side=0):
        ref = up_buf.at[zz * 2 + lax.rem(y + side, 2)]
        return rc(ref, ref, upy, zz, y_sp, t)

    def cols_of(p):
        if pieces == 1:
            return pl.ds(0, pw)
        return pl.ds(p * pw if isinstance(p, int) else pl.multiple_of(p * pw, pw), pw)

    def dn_z(zz, p):
        return rc(
            dn_ref.at[dn_rows(zz % 2), cols_of(p)], dn_buf.at[s, :, cols_of(p)],
            dnz, zz * pieces + p, zz * 2 + y, t, z * pieces + p,
        )

    def dn_zin(zz, p):
        ref = dn_buf.at[zz * 2 + y, :, cols_of(p)]
        return rc(ref, ref, dnz, 0, y_sp, t, zz * pieces + p)

    def dn_y0(p):
        return rc(
            dn_ref.at[dn_rows(zl), cols_of(p)], dn_buf.at[s, :, cols_of(p)], dny, z * pieces + p, y_sp, t
        )

    def dn_y(zz, p, side=0):
        ref = dn_buf.at[zz * 2 + lax.rem(y + side, 2), :, cols_of(p)]
        return rc(ref, ref, dny, zz * pieces + p, y_sp, t)

    def ow_x(k):
        return rc(ow_ref, ow_buf.at[t], owx, k, s, lax.rem(x + k, nth) * 2 + c)

    def ow_s0():
        return rc(ow_ref, ow_buf.at[t], ows, 0, s, sib_t)

    def ow_s(k):
        b = lax.rem(x + nth - k, nth) * 2 + c
        return rc(ow_buf.at[b], ow_buf.at[b], ows, k, s, sib_t)

    def st_c(k):
        td = lax.rem(t + k, ntp)
        return rc(st_ref.at[rows_of(td), :], st_buf.at[t], sts, k, s, td)

    def at_cols():
        return pl.ds(pl.multiple_of(y * vd, vd), vd)

    def at_c(i, tt):
        rows = pl.ds((i * ntp + tt) * share, share)
        return rc(
            at_snd.at[rows, :], at_buf.at[head_t, :, at_cols()], ats, i * ntp + tt,
            (zh * 2 + i) * 2 + c, tt, head_t * 2 + y,
        )

    def at_in(hd):
        ref = at_buf.at[hd // 2, :, pl.ds((hd % 2) * vd, vd)]
        return rc(ref, ref, ats, 0, y_sp, t, hd)

    def grp_dev(g):
        return (zh * 2 + g // nth) * 2 + y, lax.rem(g, nth) * 2 + c

    def h_rows(side, g, n):
        return h_buf.at[side, g, pl.ds(n * (share // 2), share // 2), :]

    def own_rows(n):
        return h_own.at[pl.ds(n * (share // 2), share // 2), :]

    def h_z(n):
        return rc(own_rows(n), h_rows(c, grp, n), hps, n, mate * 2 + y, t, grp * 2 + n)

    def h_x(k, n):
        dest = lax.rem(x + k, nth) * 2 + c
        return rc(own_rows(n), h_rows(c, grp, n), hps, k * 2 + n, s, dest, grp * 2 + n)

    def h_far(k, n):
        g = (1 - zl) * nth + x
        ref = h_rows(c, g, n)
        return rc(ref, ref, hps, (nth + k) * 2 + n, s, lax.rem(x + k, nth) * 2 + c, g * 2 + n)

    def h_in(zz, k, n):
        g = zz * nth + lax.rem(x + nth - k, nth)
        ref = h_rows(c, g, n)
        return rc(ref, ref, hps, 0, y_sp, t, g * 2 + n)

    def h_s0(n):
        return rc(own_rows(n), h_rows(c, grp, n), hss, grp * 2 + n, s, sib_t)

    def h_s(zz, k, n, side=0):
        g = zz * nth + lax.rem(x + nth - k, nth)
        ref = h_rows(jnp.where(side == 0, c, 1 - c), g, n)
        return rc(ref, ref, hss, g * 2 + n, s, sib_t)

    def sib_c(n):
        return rc(sib_snd.at[n], sib_buf.at[n], sbs, n, s, sib_t)

    def red_c(n, k):
        g = lax.rem(grp + k, ng)
        sp, tp = grp_dev(g)
        return rc(red_snd.at[n, g], red_buf.at[n, grp], rds, n * ng + k, sp, tp)

    def other(q, m):
        r = lax.rem(zh + q, npair)
        return r * 2 + jnp.where(r > zh, m, 1 - m)

    def shared(zz):
        return (zz > z) == (mate > z)

    inner = jnp.logical_not(shared(other(1, 0))) if npair > 1 else z < 0

    def others(fn):
        for m in range(2):
            each(1, npair, lambda q: fn(other(q, m)))

    barrier = pltpu.get_barrier_semaphore()

    def greet(sp, tp):
        pl.semaphore_signal(barrier, inc=1, device_id={"sp": sp, "tp": tp}, device_id_type=MESH)

    for o in range(4 * ntp):
        sp, tt = zh * 4 + o // ntp, o % ntp
        pl.when((sp != s) | (tt != t))(functools.partial(greet, sp, tt))

    def greet_far(q):
        for o in range(8):
            greet(lax.rem(zh + q, npair) * 4 + o // 2, x * 2 + o % 2)

    each(1, npair, greet_far)

    for ld in qk_loads:
        ld.wait()
    for j in range(heads):
        at = slice(j * qk, (j + 1) * qk)
        qsl[j] = jnp.concatenate([qin[0, :, at], qin[1, :, at]], axis=1)
        slab[j, :, :qw] = jnp.concatenate([kin[0, :, at], kin[1, :, at]], axis=1)
        lam_all[c, j] = jnp.full(lam_all.shape[2:], lam_ref[0, j], F32)
    for ld in v_loads:
        ld.wait()
    pl.semaphore_wait(barrier, 4 * ntp - 1 + 8 * (npair - 1))

    for j in range(heads):
        pl.when(jnp.logical_not(to_self(j)))(lambda: q_c(j).start())
    kv_out(lambda cp: cp.start(), True)
    kv_out(lambda cp: cp.start(), False)
    for j in range(heads):
        @pl.when(to_self(j))
        def _():
            q_buf[zl] = qsl[j]
            kv_buf[s] = slab[j]

    lam_c().start()
    each(1, ntp, lambda k: st_c(k).start())
    each(1, nth, lambda k: ow_x(k).start())
    ow_s0().start()
    def up_late():
        each(1, npair, lambda q: up_z(other(q, 1)).start())

    up_y0().start()
    up_z(mate).start()
    each(1, npair, lambda q: up_z(other(q, 0)).start())
    pl.when(inner)(lambda: up_late())
    for p in range(pieces):
        dn_y0(p).start()

    def dn_mate(early):
        @pl.when(inner == early)
        def _():
            for p in range(pieces):
                dn_z(mate, p).start()

    dn_mate(True)
    for ld in gain_loads + [st_load, ow_load, up_load, dn_load]:
        ld.start()

    m_run[...] = jnp.full(m_run.shape, -1e30, F32)
    l_run[...] = jnp.zeros(l_run.shape, F32)
    acc[...] = jnp.zeros(acc.shape, F32)
    scale = qk ** (-0.5)
    lane = lax.broadcasted_iota(jnp.int32, (tok, qw), 1)
    for i in range(2):
        pl.when(jnp.logical_not(self_worker & (zl == i)))(lambda: q_in(i).wait_recv())
        qv = q_buf[i].astype(F32) * scale
        for mp in range(2):
            keep = (lane >= mp * qk) & (lane < (mp + 1) * qk)
            qm[mp, i * tok : (i + 1) * tok, :] = jnp.where(keep, qv, 0.0).astype(BF16)

    def absorb(block):
        v = block[:, qw:]
        for r in range(2):
            sc = lax.dot_general(block[:, :qw], qm[r], NT, preferred_element_type=F32)
            old = m_run[r]
            new = jnp.maximum(old, jnp.max(sc, axis=0, keepdims=True))
            fac = jnp.exp(old - new)
            ex = jnp.exp(sc - new)
            l_run[r] = l_run[r] * fac + jnp.sum(ex, axis=0, keepdims=True)
            acc[r] = acc[r] * fac + lax.dot_general(
                v, ex.astype(BF16), TN, preferred_element_type=F32
            )
            m_run[r] = new

    def step(i, carry):
        zz = lax.rem(zh * 2 + i // 2, nz)
        own = lax.rem(i, 2) == 0

        @pl.when(own)
        def _():
            pl.when(jnp.logical_not(self_worker & (zz == z)))(lambda: kv_in(zz).wait_recv())
            kv_s(zz, c).start()

        pl.when(jnp.logical_not(own))(lambda: kv_s(zz, 1 - c).wait_recv())
        absorb(kv_buf.at[zz * 2 + jnp.where(own, c, 1 - c)])
        return carry

    lax.fori_loop(0, nsp, step, 0)

    for ld in gain_loads:
        ld.wait()
    lam_c().wait_recv()
    lam = lam_all[zl, y][:, :1]
    mixed = acc[0] / l_run[0] - lam * (acc[1] / l_run[1])
    inv = lax.rsqrt(jnp.mean(jnp.square(mixed), axis=0, keepdims=True) + 1e-05)
    normed = jnp.transpose(mixed * inv) * hg[...] * 0.8
    at_snd[...] = normed.astype(BF16)
    spots = [(i, tt) for i in range(2) for tt in range(ntp)]

    def at_mine(i, tt):
        return (i == zl) & (y == c) & (tt == t)

    for i, tt in spots:
        pl.when(jnp.logical_not(at_mine(i, tt)))(lambda: at_c(i, tt).start())

        @pl.when(at_mine(i, tt))
        def _():
            n = (i * ntp + tt) * share
            at_buf[head_t, :, at_cols()] = at_snd[n : n + share, :]

    def up_fwd(zz):
        up_zin(zz).wait_recv()
        up_y(zz).start()

    def near_fwd():
        each(1, npair, lambda q: up_fwd(other(q, 0)))

    def far_fwd():
        each(1, npair, lambda q: up_fwd(other(q, 1)))

    pl.when(jnp.logical_not(inner))(lambda: up_late())
    up_fwd(mate)
    for k in range(1, nth):
        ow_x(k).wait_recv()
        ow_s(k).start()
    st_load.wait()
    each(1, ntp, lambda k: st_c(k).wait_recv())
    cols = st_ref.shape[1]
    for b in range(ntp):
        pre[:, b * cols : (b + 1) * cols] = ALPHA * st_buf[b].astype(F32)
    for hd in range(2 * ntp):
        pl.when((y != c) | (head_t * 2 + y != hd))(lambda: at_in(hd).wait_recv())
    ow_load.wait()
    ow_s0().wait_recv()
    for k in range(1, nth):
        ow_s(k).wait_recv()
    pl.when(inner)(lambda: near_fwd())
    for b in range(ntp):
        at = slice(b * cols, (b + 1) * cols)
        tot = pre[:, at]
        for tt in range(ntp):
            tot += jnp.dot(at_buf[tt], ow_buf[tt, :, at], preferred_element_type=F32)
        pre[:, at] = tot
    h_own[...] = layer_norm(pre[...], g1[...]).astype(BF16)
    for n in range(2):
        h_z(n).start()
        for k in range(1, nth):
            h_x(k, n).start()
        h_s0(n).start()
    dn_mate(False)
    for p in range(pieces):
        others(lambda zz: dn_z(zz, p).start())
    h_buf[c, grp] = h_own[...]
    pl.when(jnp.logical_not(inner))(lambda: near_fwd())
    far_fwd()

    for n in range(2):
        h_in(1 - zl, 0, n).wait_recv()
        for k in range(1, nth):
            h_far(k, n).start()
        h_s(1 - zl, 0, n).start()
    for n in range(2):
        for k in range(1, nth):
            h_in(zl, k, n).wait_recv()
            h_s(zl, k, n).start()
    for n in range(2):
        for k in range(1, nth):
            h_in(1 - zl, k, n).wait_recv()
            h_s(1 - zl, k, n).start()
    up_load.wait()
    each(0, nz, lambda zz: up_y(zz, 1).wait_recv())
    for side in range(2):
        for k in range(nth):
            for n in range(2):
                h_s(side, k, n, 1).wait_recv()

    half = ng * share
    for side in range(2):
        parts = 2 if fh % 256 == 0 else 1
        for n in range(parts):
            wide = fh // parts
            at = slice(n * wide, (n + 1) * wide)
            hid = h_buf[side].reshape(half, d)
            w = up_buf[:, :, at].reshape(d, wide)
            up = jnp.dot(hid, w, preferred_element_type=F32)
            act[side, :, at] = jnp.square(jnp.maximum(up, 0.0)).astype(BF16)

    dn_load.wait()

    def unit(u):
        w = u // pieces
        return jnp.where(w == 0, z, jnp.where(w == 1, mate, other(w // 2, lax.rem(w, 2))))

    def finish(n):
        sib_c(n).wait_recv()
        for k in range(ng - 1, 0, -1):
            g = lax.rem(grp + k, ng)
            rows = pl.ds(pl.multiple_of(g * share, share), share)
            red_snd[n, g] = (part[n, :, rows, :] + sib_buf[n, :, rows, :].astype(F32)).astype(BF16)
            red_c(n, k).start()
        rows = pl.ds(pl.multiple_of(grp * share, share), share)
        own_part[n] = part[n, :, rows, :] + sib_buf[n, :, rows, :].astype(F32)

    def down(i, carry):
        @pl.when((i >= pieces) & (i < nz * pieces))
        def _():
            zz, p = unit(i), lax.rem(i, pieces)
            dn_zin(zz, p).wait_recv()
            dn_y(zz, p).start()

        @pl.when(i > 1)
        def _():
            finish(unit(i - 2) * pieces + lax.rem(i - 2, pieces))

        @pl.when(i > 0)
        def _():
            zz, p = unit(i - 1), lax.rem(i - 1, pieces)
            n = zz * pieces + p
            dn_y(zz, p, 1).wait_recv()
            at = cols_of(p)
            for yy in range(2):
                res = jnp.dot(act[1 - c], dn_buf[zz * 2 + yy, :, at], preferred_element_type=F32)
                sib_snd[n, yy] = res.astype(BF16)
            sib_c(n).start()
            for yy in range(2):
                part[n, yy] = jnp.dot(act[c], dn_buf[zz * 2 + yy, :, at], preferred_element_type=F32)

        return carry

    lax.fori_loop(0, nz * pieces + 1, down, 0)
    finish(unit(nz * pieces - 1) * pieces + pieces - 1)

    for zz in range(nz):
        for p in range(pieces):
            n = zz * pieces + p
            for k in range(1, ng):
                red_c(n, k).wait_recv()
            for yy in range(2):
                lo = (zz * 2 + yy) * out_w + p * pw
                at = slice(lo, lo + pw)
                tot = own_part[n, yy] + ALPHA * h_own[:, at].astype(F32)
                for k in range(ng - 1, 0, -1):
                    tot += red_buf[n, lax.rem(grp + ng - k, ng), yy].astype(F32)
                pre[:, at] = tot
    out_ref[...] = layer_norm(pre[...], g2[...]).astype(BF16)

    for j in range(heads):
        pl.when(jnp.logical_not(to_self(j)))(lambda: q_c(j).wait_send())
    kv_out(lambda cp: cp.wait_send(), False)
    kv_out(lambda cp: cp.wait_send(), True)
    for i, tt in spots:
        pl.when(jnp.logical_not(at_mine(i, tt)))(lambda: at_c(i, tt).wait_send())

    def sent(zz):
        up_z(zz).wait_send()
        up_y(zz).wait_send()
        for p in range(pieces):
            dn_z(zz, p).wait_send()
            dn_y(zz, p).wait_send()

    others(sent)
    sent(mate)
    up_y0().wait_send()
    for p in range(pieces):
        dn_y0(p).wait_send()
    each(0, nz, lambda zz: kv_s(zz, c).wait_send())
    lam_c().wait_send()
    ow_s0().wait_send()
    for n in range(2):
        h_z(n).wait_send()
        h_s0(n).wait_send()
        for k in range(1, nth):
            h_x(k, n).wait_send()
            h_far(k, n).wait_send()
            h_s(zl, k, n).wait_send()
        for k in range(nth):
            h_s(1 - zl, k, n).wait_send()
    each(0, nz * pieces, lambda n: [sib_c(n).wait_send()] + [red_c(n, k).wait_send() for k in range(1, ng)])
    for first, last, fns in ((1, nth, (ow_x, ow_s)), (1, ntp, (st_c,))):
        each(first, last, lambda k: [f(k).wait_send() for f in fns])


def local(nsp, ntp, q1, q2, k1, k2, vals, lam, hg, stream, ow, g1, up, dn, g2):
    tok = q1.shape[0]
    heads = lam.shape[0]
    hv = vals.shape[1]
    vd = hv // heads
    d = ow.shape[1]
    nz, nth = nsp // 2, ntp // 2
    ng = 2 * nth
    share = tok // ntp
    fh = up.shape[1] // 2
    qk = q1.shape[1] // heads
    half, out_w = ng * share, dn.shape[1]
    pieces = 2 if out_w % 256 == 0 else 1
    units, pw = nz * pieces, out_w // pieces
    vm = pl.BlockSpec(memory_space=pltpu.VMEM)
    sm = pl.BlockSpec(memory_space=pltpu.SMEM)
    hbm = pl.BlockSpec(memory_space=pl.ANY)
    sem = lambda n: pltpu.SemaphoreType.DMA((2, n))
    return pl.pallas_call(
        functools.partial(kernel, nsp, ntp, heads, pieces),
        out_shape=jax.ShapeDtypeStruct((share, d), BF16),
        in_specs=[sm] + [hbm] * 12,
        out_specs=vm,
        scratch_shapes=[
            pltpu.VMEM((2, heads, 1, 128), F32),
            pltpu.VMEM((2, tok, heads * qk), BF16),
            pltpu.VMEM((2, tok, heads * qk), BF16),
            pltpu.VMEM((heads, tok, 2 * qk), BF16),
            pltpu.VMEM((heads, tok, 2 * qk + vd), BF16),
            pltpu.VMEM((1, vd), F32),
            pltpu.VMEM((1, d), F32),
            pltpu.VMEM((1, d), F32),
            pltpu.VMEM((2, tok, 2 * qk), BF16),
            pltpu.VMEM((2, 2 * tok, 2 * qk), BF16),
            pltpu.VMEM((2, 1, 2 * tok), F32),
            pltpu.VMEM((2, 1, 2 * tok), F32),
            pltpu.VMEM((2, vd, 2 * tok), F32),
            pltpu.VMEM((nsp, tok, 2 * qk + vd), BF16),
            pltpu.VMEM((nsp, up.shape[0], fh), BF16),
            pltpu.VMEM((nsp, fh, out_w), BF16),
            pltpu.VMEM((ntp,) + ow.shape, BF16),
            pltpu.VMEM((ntp, share, stream.shape[1]), BF16),
            pltpu.VMEM((2 * tok, vd), BF16),
            pltpu.VMEM((ntp, share, hv), BF16),
            pltpu.VMEM((share, d), F32),
            pltpu.VMEM((share, d), BF16),
            pltpu.VMEM((2, ng, share, d), BF16),
            pltpu.VMEM((2, half, fh), BF16),
            pltpu.VMEM((units, 2, half, pw), BF16),
            pltpu.VMEM((units, 2, half, pw), BF16),
            pltpu.VMEM((units, 2, half, pw), F32),
            pltpu.VMEM((units, 2, share, pw), F32),
            pltpu.VMEM((units, ng, 2, share, pw), BF16),
            pltpu.VMEM((units, ng, 2, share, pw), BF16),
            pltpu.SemaphoreType.DMA((4 + heads + 7,)),
            sem(1), sem(max(heads, 2)), sem(max(nz // 2 * heads, nz)), sem(nz),
            sem(nz), sem(nz), sem(units), sem(units),
            sem(nth), sem(nth), sem(ntp), sem(2 * ntp), sem(2 * ng), sem(2 * ng), sem(units), sem(units * ng),
        ],
        compiler_params=pltpu.CompilerParams(
            collective_id=0, has_side_effects=True, vmem_limit_bytes=60 * 1024 * 1024
        ),
    )(
        lam.reshape(1, heads), q1, q2, k1, k2, vals, hg.reshape(1, vd), stream, ow,
        g1.reshape(1, d), up, dn, g2.reshape(1, d),
    )


def solution(mesh):
    in_specs = (
        P("sp", "tp"),
        P("sp", "tp"),
        P("sp", "tp"),
        P("sp", "tp"),
        P("sp", "tp"),
        P("tp"),
        P(),
        P("sp", "tp"),
        P("tp", None),
        P(),
        P("sp", "tp"),
        P("tp", "sp"),
        P(),
    )
    body = functools.partial(local, mesh.shape["sp"], mesh.shape["tp"])
    return jax.shard_map(
        body, mesh=mesh, in_specs=in_specs, out_specs=P(("sp", "tp"), None), check_vma=False
    )
```

```python
import functools

import jax
import jax.numpy as jnp
from jax import lax
from jax.experimental import pallas as pl
from jax.experimental.pallas import tpu as pltpu
from jax.sharding import PartitionSpec as P

MESH = pl.DeviceIdType.MESH
F32, BF16 = jnp.float32, jnp.bfloat16
ALPHA = 2.0**0.5
NT = (((1,), (1,)), ((), ()))
TN = (((0,), (0,)), ((), ()))
KINDS = 13
LAM, Q, KV, KVS, UP, DN, OW, ST, AT, HP, HS, SIB, RED = range(KINDS)


def layer_norm(value, gain):
    centre = jnp.mean(value, axis=-1, keepdims=True)
    spread = jnp.mean(jnp.square(value - centre), axis=-1, keepdims=True)
    return (value - centre) * lax.rsqrt(spread + 1e-05) * gain


def kernel(
    nsp, ntp, heads, pieces,
    lam_ref, q1_ref, q2_ref, k1_ref, k2_ref, v_ref, hg_ref, st_ref, ow_ref, g1_ref, up_ref, dn_ref, g2_ref,
    out_ref,
    lam_all, qin, kin, qsl, slab, hg, g1, g2,
    q_buf, qm, m_run, l_run, acc, kv_buf, up_buf, dn_buf, ow_buf, st_buf, at_snd, at_buf,
    pre, h_own, h_buf, act, sib_snd, sib_buf, part, own_part, red_snd, red_buf,
    loc_sem, snd, one, rq, rkv, rkvs, rup, rdz, rdy, rox, rh, rsib, rred,
):
    s, t = lax.axis_index("sp"), lax.axis_index("tp")
    nz, nth = nsp // 2, ntp // 2
    npair = nz // 2
    ng = 2 * nth
    z, y = s // 2, s % 2
    zh, zl = z // 2, z % 2
    mate = zh * 2 + 1 - zl
    x, c = t // 2, t % 2
    sib_t = x * 2 + (1 - c)
    y_sp = z * 2 + (1 - y)
    grp = zl * nth + x
    tok = q1_ref.shape[0]
    share = tok // ntp
    fh = up_ref.shape[1] // 2
    vd = acc.shape[1]
    qw = q_buf.shape[2]
    qk = qw // 2
    d = pre.shape[1]
    out_w = dn_buf.shape[2]
    pw = out_w // pieces
    head_t = x * 2 + zl

    def rc(src, dst, kind, arrive, sp, tp):
        return pltpu.make_async_remote_copy(
            src_ref=src, dst_ref=dst, send_sem=snd.at[kind], recv_sem=arrive,
            device_id={"sp": sp, "tp": tp}, device_id_type=MESH,
        )

    def arrived(ref, sem):
        rc(ref, ref, 0, sem, y_sp, t).wait_recv()

    def left(ref, kind):
        rc(ref, ref, kind, one.at[LAM], y_sp, t).wait_send()

    def each(lo, hi, body):
        if hi - lo <= 4:
            for k in range(lo, hi):
                body(k)
        else:
            lax.fori_loop(lo, hi, lambda k, carry: (body(k), carry)[1], 0)

    def lc(src, dst, i):
        return pltpu.make_async_copy(src, dst, loc_sem.at[i])

    def up_half(j):
        return up_ref.at[:, pl.ds(pl.multiple_of(j * fh, fh), fh)]

    def dn_rows(j):
        return pl.ds(pl.multiple_of(j * fh, fh), fh)

    def rows_of(tt):
        return pl.ds(pl.multiple_of(tt * share, share), share)

    qk_loads = [
        lc(q1_ref, qin.at[0], 0),
        lc(q2_ref, qin.at[1], 1),
        lc(k1_ref, kin.at[0], 2),
        lc(k2_ref, kin.at[1], 3),
    ]
    v_loads = [
        lc(v_ref.at[:, pl.ds(j * vd, vd)], slab.at[j, :, pl.ds(qw, vd)], 4 + j) for j in range(heads)
    ]
    n0 = 4 + heads
    gain_loads = [lc(hg_ref, hg, n0), lc(g1_ref, g1, n0 + 1), lc(g2_ref, g2, n0 + 2)]
    up_load = lc(up_half(zl), up_buf.at[s], n0 + 3)
    dn_load = lc(dn_ref.at[dn_rows(zl), :], dn_buf.at[s], n0 + 4)
    ow_load = lc(ow_ref, ow_buf.at[t], n0 + 5)
    st_load = lc(st_ref.at[rows_of(t), :], st_buf.at[t], n0 + 6)
    for ld in qk_loads + v_loads:
        ld.start()

    def lam_c():
        return rc(lam_all.at[c], lam_all.at[c], LAM, one.at[LAM], s, sib_t)

    def to_self(j):
        return (c == zl) & (y == c) & (j == y)

    self_worker = (c == zl) & (y == c)

    def q_c(j):
        return rc(qsl.at[j], q_buf.at[zl], Q, rq.at[zl], (zh * 2 + c) * 2 + j, x * 2 + y)

    def kv_c(r, j):
        return rc(slab.at[j], kv_buf.at[s], KV, rkv.at[z], (r * 2 + c) * 2 + j, x * 2 + y)

    def kv_s(zz):
        ref = kv_buf.at[zz * 2 + c]
        return rc(ref, ref, KVS, rkvs.at[zz], s, sib_t)

    def kv_out(fn, own):
        for j in range(heads):
            if own:
                pl.when(jnp.logical_not(to_self(j)))(lambda: fn(kv_c(zh, j)))
            else:
                each(1, npair, lambda q: fn(kv_c(lax.rem(zh + q, npair), j)))

    ur = up_ref.shape[0] // 2

    def up_rows(p):
        return pl.ds(p * ur, ur)

    def up_part(j, p):
        return up_ref.at[up_rows(p), pl.ds(pl.multiple_of(j * fh, fh), fh)]

    def up_z(zz, p):
        return rc(up_part(zz % 2, p), up_buf.at[s, up_rows(p)], UP, rup.at[z * 2 + p], zz * 2 + y, t)

    def up_y0(p):
        return rc(up_part(zl, p), up_buf.at[s, up_rows(p)], UP, one.at[UP], y_sp, t)

    def up_fwd(zz, p):
        ref = up_buf.at[zz * 2 + y, up_rows(p)]
        arrived(ref, rup.at[zz * 2 + p])
        rc(ref, ref, UP, one.at[UP], y_sp, t).start()

    def cols_of(p):
        if pieces == 1:
            return pl.ds(0, pw)
        return pl.ds(p * pw if isinstance(p, int) else pl.multiple_of(p * pw, pw), pw)

    def dn_part(j, p):
        return dn_ref.at[dn_rows(j), cols_of(p)]

    def dn_z(zz, p):
        return rc(
            dn_part(zz % 2, p), dn_buf.at[s, :, cols_of(p)], DN, rdz.at[z * pieces + p], zz * 2 + y, t
        )

    def dn_y0(p):
        return rc(dn_part(zl, p), dn_buf.at[s, :, cols_of(p)], DN, rdy.at[z * pieces + p], y_sp, t)

    def dn_fwd(zz, p):
        ref = dn_buf.at[zz * 2 + y, :, cols_of(p)]
        arrived(ref, rdz.at[zz * pieces + p])
        rc(ref, ref, DN, rdy.at[zz * pieces + p], y_sp, t).start()

    def ow_x(k):
        return rc(ow_ref, ow_buf.at[t], OW, rox.at[k], s, lax.rem(x + k, nth) * 2 + c)

    def ow_s0():
        return rc(ow_ref, ow_buf.at[t], OW, one.at[OW], s, sib_t)

    def ow_fwd(k):
        ref = ow_buf.at[lax.rem(x + nth - k, nth) * 2 + c]
        arrived(ref, rox.at[k])
        rc(ref, ref, OW, one.at[OW], s, sib_t).start()

    def st_c(k):
        td = lax.rem(t + k, ntp)
        return rc(st_ref.at[rows_of(td), :], st_buf.at[t], ST, one.at[ST], s, td)

    def at_cols():
        return pl.ds(pl.multiple_of(y * vd, vd), vd)

    def at_c(i, tt):
        rows = pl.ds((i * ntp + tt) * share, share)
        return rc(
            at_snd.at[rows, :], at_buf.at[head_t, :, at_cols()], AT, one.at[AT], (zh * 2 + i) * 2 + c, tt
        )

    def at_all(fn):
        pl.when(y == c)(lambda: fn(at_snd.at[pl.ds(0, 2 * tok - share)]))
        pl.when(y != c)(lambda: fn(at_snd.at[pl.ds(0, 2 * tok)]))

    def grp_dev(g):
        return (zh * 2 + g // nth) * 2 + y, lax.rem(g, nth) * 2 + c

    def h_rows(g, n):
        return h_buf.at[c, g, pl.ds(n * (share // 2), share // 2), :]

    def own_rows(n):
        return h_own.at[pl.ds(n * (share // 2), share // 2), :]

    def h_z(n):
        return rc(own_rows(n), h_rows(grp, n), HP, rh.at[grp * 2 + n], mate * 2 + y, t)

    def h_x(k, n):
        dest = lax.rem(x + k, nth) * 2 + c
        return rc(own_rows(n), h_rows(grp, n), HP, rh.at[grp * 2 + n], s, dest)

    def h_s0(n):
        return rc(own_rows(n), h_rows(grp, n), HS, one.at[HS], s, sib_t)

    def h_fwd(zz, k, n, far=False):
        g = zz * nth + lax.rem(x + nth - k, nth)
        ref = h_rows(g, n)
        arrived(ref, rh.at[g * 2 + n])
        if far:
            for i in range(1, nth):
                rc(ref, ref, HP, rh.at[g * 2 + n], s, lax.rem(x + i, nth) * 2 + c).start()
        rc(ref, ref, HS, one.at[HS], s, sib_t).start()

    def sib_c(n):
        return rc(sib_snd.at[n], sib_buf.at[n], SIB, rsib.at[n], s, sib_t)

    def red_c(n, k):
        g = lax.rem(grp + k, ng)
        sp, tp = grp_dev(g)
        return rc(red_snd.at[n, g], red_buf.at[n, grp], RED, rred.at[n], sp, tp)

    def other(q, m):
        r = lax.rem(zh + q, npair)
        return r * 2 + jnp.where(r > zh, m, 1 - m)

    def shared(zz):
        return (zz > z) == (mate > z)

    inner = jnp.logical_not(shared(other(1, 0))) if npair > 1 else z < 0

    def others(fn):
        for m in range(2):
            each(1, npair, lambda q: fn(other(q, m)))

    barrier = pltpu.get_barrier_semaphore()

    def greet(sp, tp):
        pl.semaphore_signal(barrier, inc=1, device_id={"sp": sp, "tp": tp}, device_id_type=MESH)

    for o in range(4 * ntp):
        sp, tt = zh * 4 + o // ntp, o % ntp
        pl.when((sp != s) | (tt != t))(functools.partial(greet, sp, tt))

    def greet_far(q):
        for o in range(8):
            greet(lax.rem(zh + q, npair) * 4 + o // 2, x * 2 + o % 2)

    each(1, npair, greet_far)

    for ld in qk_loads:
        ld.wait()
    for j in range(heads):
        at = slice(j * qk, (j + 1) * qk)
        qsl[j] = jnp.concatenate([qin[0, :, at], qin[1, :, at]], axis=1)
        slab[j, :, :qw] = jnp.concatenate([kin[0, :, at], kin[1, :, at]], axis=1)
        lam_all[c, j] = jnp.full(lam_all.shape[2:], lam_ref[0, j], F32)
    for ld in v_loads:
        ld.wait()
    pl.semaphore_wait(barrier, 4 * ntp - 1 + 8 * (npair - 1))

    for j in range(heads):
        pl.when(jnp.logical_not(to_self(j)))(lambda: q_c(j).start())
    kv_out(lambda cp: cp.start(), True)
    kv_out(lambda cp: cp.start(), False)
    for j in range(heads):
        @pl.when(to_self(j))
        def _():
            q_buf[zl] = qsl[j]
            kv_buf[s] = slab[j]

    lam_c().start()
    each(1, nth, lambda k: ow_x(k).start())
    each(1, ntp, lambda k: st_c(k).start())
    ow_s0().start()
    def up_far(p):
        each(1, npair, lambda q: up_z(other(q, 1), p).start())
        each(1, npair, lambda q: up_z(other(q, 0), p).start())

    for p in range(2):
        up_y0(p).start()
    for p in range(2):
        up_z(mate, p).start()
    up_far(0)
    pl.when(inner)(lambda: up_far(1))
    for p in range(pieces):
        dn_y0(p).start()
    for ld in gain_loads + [st_load, ow_load, up_load, dn_load]:
        ld.start()

    m_run[...] = jnp.full(m_run.shape, -1e30, F32)
    l_run[...] = jnp.zeros(l_run.shape, F32)
    acc[...] = jnp.zeros(acc.shape, F32)
    scale = qk ** (-0.5)
    lane = lax.broadcasted_iota(jnp.int32, (tok, qw), 1)
    for i in range(2):
        pl.when(jnp.logical_not(self_worker & (zl == i)))(lambda: arrived(q_buf.at[i], rq.at[i]))
        qv = q_buf[i].astype(F32) * scale
        for mp in range(2):
            keep = (lane >= mp * qk) & (lane < (mp + 1) * qk)
            qm[mp, i * tok : (i + 1) * tok, :] = jnp.where(keep, qv, 0.0).astype(BF16)

    def absorb(block):
        v = block[:, qw:]
        for r in range(2):
            sc = lax.dot_general(block[:, :qw], qm[r], NT, preferred_element_type=F32)
            old = m_run[r]
            new = jnp.maximum(old, jnp.max(sc, axis=0, keepdims=True))
            fac = jnp.exp(old - new)
            ex = jnp.exp(sc - new)
            l_run[r] = l_run[r] * fac + jnp.sum(ex, axis=0, keepdims=True)
            acc[r] = acc[r] * fac + lax.dot_general(
                v, ex.astype(BF16), TN, preferred_element_type=F32
            )
            m_run[r] = new

    def step(i, carry):
        zz = lax.rem(zh * 2 + i // 2, nz)
        own = lax.rem(i, 2) == 0

        @pl.when(own)
        def _():
            direct = kv_buf.at[zz * 2 + c]
            pl.when(jnp.logical_not(self_worker & (zz == z)))(lambda: arrived(direct, rkv.at[zz]))
            kv_s(zz).start()

        pl.when(jnp.logical_not(own))(lambda: arrived(kv_buf.at[zz * 2 + 1 - c], rkvs.at[zz]))
        absorb(kv_buf.at[zz * 2 + jnp.where(own, c, 1 - c)])
        return carry

    lax.fori_loop(0, nsp, step, 0)

    for ld in gain_loads:
        ld.wait()
    arrived(lam_all.at[c], one.at[LAM])
    lam = lam_all[zl, y][:, :1]
    mixed = acc[0] / l_run[0] - lam * (acc[1] / l_run[1])
    inv = lax.rsqrt(jnp.mean(jnp.square(mixed), axis=0, keepdims=True) + 1e-05)
    normed = jnp.transpose(mixed * inv) * hg[...] * 0.8
    at_snd[...] = normed.astype(BF16)
    spots = [(i, tt) for i in range(2) for tt in range(ntp)]

    def at_mine(i, tt):
        return (i == zl) & (y == c) & (tt == t)

    for i, tt in spots:
        pl.when(jnp.logical_not(at_mine(i, tt)))(lambda: at_c(i, tt).start())

        @pl.when(at_mine(i, tt))
        def _():
            n = (i * ntp + tt) * share
            at_buf[head_t, :, at_cols()] = at_snd[n : n + share, :]

    def others_fwd(p):
        each(1, npair, lambda q: [up_fwd(other(q, m), p) for m in range(2)])

    pl.when(jnp.logical_not(inner))(lambda: up_far(1))
    for p in range(2):
        up_fwd(mate, p)
    for k in range(1, nth):
        ow_fwd(k)
    others_fwd(0)
    st_load.wait()
    arrived(st_buf.at[pl.ds(0, ntp - 1)], one.at[ST])
    cols = st_ref.shape[1]
    for b in range(ntp):
        pre[:, b * cols : (b + 1) * cols] = ALPHA * st_buf[b].astype(F32)
    at_all(lambda ref: arrived(ref, one.at[AT]))
    ow_load.wait()
    arrived(ow_buf.at[pl.ds(0, nth)], one.at[OW])
    for b in range(ntp):
        at = slice(b * cols, (b + 1) * cols)
        tot = pre[:, at]
        for tt in range(ntp):
            tot += jnp.dot(at_buf[tt], ow_buf[tt, :, at], preferred_element_type=F32)
        pre[:, at] = tot
    h_own[...] = layer_norm(pre[...], g1[...]).astype(BF16)
    for n in range(2):
        h_z(n).start()
        for k in range(1, nth):
            h_x(k, n).start()
        h_s0(n).start()
    for p in range(pieces):
        dn_z(mate, p).start()
    for p in range(pieces):
        each(1, npair, lambda q: dn_z(other(q, 0), p).start())
    h_buf[c, grp] = h_own[...]
    others_fwd(1)

    for n in range(2):
        h_fwd(1 - zl, 0, n, True)
    for p in range(pieces):
        each(1, npair, lambda q: dn_z(other(q, 1), p).start())
    for zz in (zl, 1 - zl):
        for n in range(2):
            for k in range(1, nth):
                h_fwd(zz, k, n)
    up_load.wait()
    arrived(up_buf.at[pl.ds(0, nz)], one.at[UP])
    arrived(h_buf.at[0], one.at[HS])

    half = ng * share
    for side in range(2):
        parts = 2 if fh % 256 == 0 else 1
        for n in range(parts):
            wide = fh // parts
            at = slice(n * wide, (n + 1) * wide)
            hid = h_buf[side].reshape(half, d)
            w = up_buf[:, :, at].reshape(d, wide)
            up = jnp.dot(hid, w, preferred_element_type=F32)
            act[side, :, at] = jnp.square(jnp.maximum(up, 0.0)).astype(BF16)
    dn_load.wait()

    steps = nz * pieces

    def unit(i):
        r = lax.rem(i, 2 * pieces)
        far = other(i // (2 * pieces), lax.rem(r, 2))
        zz = jnp.where(i < pieces, z, jnp.where(i < 2 * pieces, mate, far))
        return zz, jnp.where(i < 2 * pieces, lax.rem(i, pieces), r // 2)

    def index(i):
        zz, p = unit(i)
        return zz * pieces + p

    def finish(n):
        arrived(sib_buf.at[n], rsib.at[n])
        for k in range(ng - 1, 0, -1):
            g = lax.rem(grp + k, ng)
            rows = pl.ds(pl.multiple_of(g * share, share), share)
            red_snd[n, g] = (part[n, :, rows, :] + sib_buf[n, :, rows, :].astype(F32)).astype(BF16)
            red_c(n, k).start()
        rows = pl.ds(pl.multiple_of(grp * share, share), share)
        own_part[n] = part[n, :, rows, :] + sib_buf[n, :, rows, :].astype(F32)

    ahead, lead = pieces, 2

    def down(i, carry):
        pl.when((i + lead >= ahead) & (i + lead < steps))(lambda: dn_fwd(*unit(i + lead)))
        pl.when(i > 0)(lambda: finish(index(i - 1)))
        zz, p = unit(i)
        n = zz * pieces + p
        arrived(dn_buf.at[zz * 2 + 1 - y, :, cols_of(p)], rdy.at[n])
        at = cols_of(p)
        for yy in range(2):
            res = jnp.dot(act[1 - c], dn_buf[zz * 2 + yy, :, at], preferred_element_type=F32)
            sib_snd[n, yy] = res.astype(BF16)
        sib_c(n).start()
        for yy in range(2):
            part[n, yy] = jnp.dot(act[c], dn_buf[zz * 2 + yy, :, at], preferred_element_type=F32)
        return carry

    lax.fori_loop(0, steps, down, 0)
    finish(index(steps - 1))

    for zz in range(nz):
        for p in range(pieces):
            n = zz * pieces + p
            arrived(red_buf.at[n, pl.ds(0, ng - 1)], rred.at[n])
            for yy in range(2):
                lo = (zz * 2 + yy) * out_w + p * pw
                at = slice(lo, lo + pw)
                tot = own_part[n, yy] + ALPHA * h_own[:, at].astype(F32)
                for k in range(ng - 1, 0, -1):
                    tot += red_buf[n, lax.rem(grp + ng - k, ng), yy].astype(F32)
                pre[:, at] = tot
    out_ref[...] = layer_norm(pre[...], g2[...]).astype(BF16)

    for kind, buf, most in ((Q, qsl, heads), (KV, kv_buf, npair * heads)):
        pl.when(self_worker)(lambda: left(buf.at[pl.ds(0, most - 1)], kind))
        pl.when(jnp.logical_not(self_worker))(lambda: left(buf.at[pl.ds(0, most)], kind))
    at_all(lambda ref: left(ref, AT))
    left(lam_all.at[c], LAM)
    left(kv_buf.at[pl.ds(0, nz)], KVS)
    left(up_buf.at[pl.ds(0, nsp - 1)], UP)
    left(dn_buf.at[pl.ds(0, nsp - 1)], DN)
    left(ow_buf.at[pl.ds(0, ntp - 1)], OW)
    left(st_buf.at[pl.ds(0, ntp - 1)], ST)
    left(h_buf.at[0, pl.ds(0, ng - 1)], HP)
    left(h_buf.at[0], HS)
    left(sib_snd, SIB)
    left(red_snd.at[:, pl.ds(0, ng - 1)], RED)


def local(nsp, ntp, q1, q2, k1, k2, vals, lam, hg, stream, ow, g1, up, dn, g2):
    tok = q1.shape[0]
    heads = lam.shape[0]
    hv = vals.shape[1]
    vd = hv // heads
    d = ow.shape[1]
    nz, nth = nsp // 2, ntp // 2
    ng = 2 * nth
    share = tok // ntp
    fh = up.shape[1] // 2
    qk = q1.shape[1] // heads
    half, out_w = ng * share, dn.shape[1]
    pieces = 2 if out_w % 256 == 0 else 1
    units, pw = nz * pieces, out_w // pieces
    vm = pl.BlockSpec(memory_space=pltpu.VMEM)
    sm = pl.BlockSpec(memory_space=pltpu.SMEM)
    hbm = pl.BlockSpec(memory_space=pl.ANY)
    sems = (KINDS, KINDS, 2, nz, nz, 2 * nz, units, units, nth, 2 * ng, units, units)
    return pl.pallas_call(
        functools.partial(kernel, nsp, ntp, heads, pieces),
        out_shape=pltpu.VMEM((share, d), BF16),
        in_specs=[sm] + [hbm] * 12,
        out_specs=vm,
        scratch_shapes=[
            pltpu.VMEM((2, heads, 1, 128), F32),
            pltpu.VMEM((2, tok, heads * qk), BF16),
            pltpu.VMEM((2, tok, heads * qk), BF16),
            pltpu.VMEM((heads, tok, 2 * qk), BF16),
            pltpu.VMEM((heads, tok, 2 * qk + vd), BF16),
            pltpu.VMEM((1, vd), F32),
            pltpu.VMEM((1, d), F32),
            pltpu.VMEM((1, d), F32),
            pltpu.VMEM((2, tok, 2 * qk), BF16),
            pltpu.VMEM((2, 2 * tok, 2 * qk), BF16),
            pltpu.VMEM((2, 1, 2 * tok), F32),
            pltpu.VMEM((2, 1, 2 * tok), F32),
            pltpu.VMEM((2, vd, 2 * tok), F32),
            pltpu.VMEM((nsp, tok, 2 * qk + vd), BF16),
            pltpu.VMEM((nsp, up.shape[0], fh), BF16),
            pltpu.VMEM((nsp, fh, out_w), BF16),
            pltpu.VMEM((ntp,) + ow.shape, BF16),
            pltpu.VMEM((ntp, share, stream.shape[1]), BF16),
            pltpu.VMEM((2 * tok, vd), BF16),
            pltpu.VMEM((ntp, share, hv), BF16),
            pltpu.VMEM((share, d), F32),
            pltpu.VMEM((share, d), BF16),
            pltpu.VMEM((2, ng, share, d), BF16),
            pltpu.VMEM((2, half, fh), BF16),
            pltpu.VMEM((units, 2, half, pw), BF16),
            pltpu.VMEM((units, 2, half, pw), BF16),
            pltpu.VMEM((units, 2, half, pw), F32),
            pltpu.VMEM((units, 2, share, pw), F32),
            pltpu.VMEM((units, ng, 2, share, pw), BF16),
            pltpu.VMEM((units, ng, 2, share, pw), BF16),
            pltpu.SemaphoreType.DMA((4 + heads + 7,)),
            *[pltpu.SemaphoreType.DMA((n,)) for n in sems],
        ],
        compiler_params=pltpu.CompilerParams(
            collective_id=0, has_side_effects=True, vmem_limit_bytes=60 * 1024 * 1024
        ),
    )(
        lam.reshape(1, heads), q1, q2, k1, k2, vals, hg.reshape(1, vd), stream, ow,
        g1.reshape(1, d), up, dn, g2.reshape(1, d),
    )


def solution(mesh):
    in_specs = (
        P("sp", "tp"),
        P("sp", "tp"),
        P("sp", "tp"),
        P("sp", "tp"),
        P("sp", "tp"),
        P("tp"),
        P(),
        P("sp", "tp"),
        P("tp", None),
        P(),
        P("sp", "tp"),
        P("tp", "sp"),
        P(),
    )
    body = functools.partial(local, mesh.shape["sp"], mesh.shape["tp"])
    return jax.shard_map(
        body, mesh=mesh, in_specs=in_specs, out_specs=P(("sp", "tp"), None), check_vma=False
    )
```

```python
import functools

import jax
import jax.numpy as jnp
from jax import lax
from jax.experimental import pallas as pl
from jax.experimental.pallas import tpu as pltpu
from jax.sharding import PartitionSpec as P

MESH = pl.DeviceIdType.MESH
F32, BF16 = jnp.float32, jnp.bfloat16
ALPHA = 2.0**0.5
NT = (((1,), (1,)), ((), ()))
TN = (((0,), (0,)), ((), ()))
KINDS = 13
LAM, Q, KV, KVS, UP, DN, OW, ST, AT, HP, HS, SIB, RED = range(KINDS)


def layer_norm(value, gain):
    centre = jnp.mean(value, axis=-1, keepdims=True)
    spread = jnp.mean(jnp.square(value - centre), axis=-1, keepdims=True)
    return (value - centre) * lax.rsqrt(spread + 1e-05) * gain


def kernel(
    nsp, ntp, heads, pieces,
    lam_ref, q1_ref, q2_ref, k1_ref, k2_ref, v_ref, hg_ref, st_ref, ow_ref, g1_ref, up_ref, dn_ref, g2_ref,
    out_ref,
    lam_in, lam_all, qin, kin, qsl, slab, hg, g1, g2,
    q_buf, qm, m_run, l_run, acc, kv_buf, up_buf, dn_buf, ow_buf, st_buf, at_snd, at_buf,
    pre, h_own, h_buf, act, sib_snd, sib_buf, part, own_part, red_snd, red_buf,
    loc_sem, snd, one, rq, rkv, rkvs, rup, rdz, rdy, rox, rh, rsib, rred,
):
    s, t = lax.axis_index("sp"), lax.axis_index("tp")
    nz, nth = nsp // 2, ntp // 2
    npair = nz // 2
    ng = 2 * nth
    z, y = s // 2, s % 2
    zh, zl = z // 2, z % 2
    mate = zh * 2 + 1 - zl
    x, c = t // 2, t % 2
    sib_t = x * 2 + (1 - c)
    y_sp = z * 2 + (1 - y)
    grp = zl * nth + x
    tok = q1_ref.shape[0]
    share = tok // ntp
    fh = up_ref.shape[1] // 2
    vd = acc.shape[1]
    qw = q_buf.shape[2]
    qk = qw // 2
    d = pre.shape[1]
    out_w = dn_buf.shape[2]
    pw = out_w // pieces
    head_t = x * 2 + zl

    def rc(src, dst, kind, arrive, sp, tp):
        return pltpu.make_async_remote_copy(
            src_ref=src, dst_ref=dst, send_sem=snd.at[kind], recv_sem=arrive,
            device_id={"sp": sp, "tp": tp}, device_id_type=MESH,
        )

    def arrived(ref, sem):
        rc(ref, ref, 0, sem, y_sp, t).wait_recv()

    def left(ref, kind):
        rc(ref, ref, kind, one.at[LAM], y_sp, t).wait_send()

    def each(lo, hi, body):
        if hi - lo <= 4:
            for k in range(lo, hi):
                body(k)
        else:
            lax.fori_loop(lo, hi, lambda k, carry: (body(k), carry)[1], 0)

    def lc(src, dst, i):
        return pltpu.make_async_copy(src, dst, loc_sem.at[i])

    def up_half(j):
        return up_ref.at[:, pl.ds(pl.multiple_of(j * fh, fh), fh)]

    def dn_rows(j):
        return pl.ds(pl.multiple_of(j * fh, fh), fh)

    def rows_of(tt):
        return pl.ds(pl.multiple_of(tt * share, share), share)

    qk_loads = [
        lc(q1_ref, qin.at[0], 0),
        lc(q2_ref, qin.at[1], 1),
        lc(k1_ref, kin.at[0], 2),
        lc(k2_ref, kin.at[1], 3),
    ]
    v_loads = [
        lc(v_ref.at[:, pl.ds(j * vd, vd)], slab.at[j, :, pl.ds(qw, vd)], 4 + j) for j in range(heads)
    ]
    n0 = 5 + heads
    lam_load = lc(lam_ref, lam_in, 4 + heads)
    gain_loads = [lc(hg_ref, hg, n0), lc(g1_ref, g1, n0 + 1), lc(g2_ref, g2, n0 + 2)]
    up_load = lc(up_half(zl), up_buf.at[s], n0 + 3)
    dn_load = lc(dn_ref.at[dn_rows(zl), :], dn_buf.at[s], n0 + 4)
    ow_load = lc(ow_ref, ow_buf.at[t], n0 + 5)
    st_load = lc(st_ref.at[rows_of(t), :], st_buf.at[t], n0 + 6)

    def lam_c():
        return rc(lam_all.at[c], lam_all.at[c], LAM, one.at[LAM], s, sib_t)

    def to_self(j):
        return (c == zl) & (y == c) & (j == y)

    self_worker = (c == zl) & (y == c)

    def q_c(j):
        return rc(qsl.at[j], q_buf.at[zl], Q, rq.at[zl], (zh * 2 + c) * 2 + j, x * 2 + y)

    def kv_c(r, j):
        return rc(slab.at[j], kv_buf.at[s], KV, rkv.at[z], (r * 2 + c) * 2 + j, x * 2 + y)

    def kv_s(zz):
        ref = kv_buf.at[zz * 2 + c]
        return rc(ref, ref, KVS, rkvs.at[zz], s, sib_t)

    def kv_out(fn, own):
        for j in range(heads):
            if own:
                pl.when(jnp.logical_not(to_self(j)))(lambda: fn(kv_c(zh, j)))
            else:
                each(1, npair, lambda q: fn(kv_c(lax.rem(zh + q, npair), j)))

    ur = up_ref.shape[0] // 2

    def up_rows(p):
        return pl.ds(p * ur, ur)

    def up_part(j, p):
        return up_ref.at[up_rows(p), pl.ds(pl.multiple_of(j * fh, fh), fh)]

    def up_z(zz, p):
        return rc(up_part(zz % 2, p), up_buf.at[s, up_rows(p)], UP, rup.at[z * 2 + p], zz * 2 + y, t)

    def up_y0(p):
        return rc(up_part(zl, p), up_buf.at[s, up_rows(p)], UP, one.at[UP], y_sp, t)

    def up_fwd(zz, p):
        ref = up_buf.at[zz * 2 + y, up_rows(p)]
        arrived(ref, rup.at[zz * 2 + p])
        rc(ref, ref, UP, one.at[UP], y_sp, t).start()

    def cols_of(p):
        if pieces == 1:
            return pl.ds(0, pw)
        return pl.ds(p * pw if isinstance(p, int) else pl.multiple_of(p * pw, pw), pw)

    def dn_part(j, p):
        return dn_ref.at[dn_rows(j), cols_of(p)]

    def dn_z(zz, p):
        return rc(
            dn_part(zz % 2, p), dn_buf.at[s, :, cols_of(p)], DN, rdz.at[z * pieces + p], zz * 2 + y, t
        )

    def dn_y0(p):
        return rc(dn_part(zl, p), dn_buf.at[s, :, cols_of(p)], DN, rdy.at[z * pieces + p], y_sp, t)

    def dn_fwd(zz, p):
        ref = dn_buf.at[zz * 2 + y, :, cols_of(p)]
        arrived(ref, rdz.at[zz * pieces + p])
        rc(ref, ref, DN, rdy.at[zz * pieces + p], y_sp, t).start()

    def ow_x(k):
        return rc(ow_ref, ow_buf.at[t], OW, rox.at[k], s, lax.rem(x + k, nth) * 2 + c)

    def ow_s0():
        return rc(ow_ref, ow_buf.at[t], OW, one.at[OW], s, sib_t)

    def ow_fwd(k):
        ref = ow_buf.at[lax.rem(x + nth - k, nth) * 2 + c]
        arrived(ref, rox.at[k])
        rc(ref, ref, OW, one.at[OW], s, sib_t).start()

    def st_c(k):
        td = lax.rem(t + k, ntp)
        return rc(st_ref.at[rows_of(td), :], st_buf.at[t], ST, one.at[ST], s, td)

    def at_cols():
        return pl.ds(pl.multiple_of(y * vd, vd), vd)

    def at_c(i, tt):
        rows = pl.ds((i * ntp + tt) * share, share)
        return rc(
            at_snd.at[rows, :], at_buf.at[head_t, :, at_cols()], AT, one.at[AT], (zh * 2 + i) * 2 + c, tt
        )

    def at_all(fn):
        pl.when(y == c)(lambda: fn(at_snd.at[pl.ds(0, 2 * tok - share)]))
        pl.when(y != c)(lambda: fn(at_snd.at[pl.ds(0, 2 * tok)]))

    def grp_dev(g):
        return (zh * 2 + g // nth) * 2 + y, lax.rem(g, nth) * 2 + c

    def h_rows(g, n):
        return h_buf.at[c, g, pl.ds(n * (share // 2), share // 2), :]

    def own_rows(n):
        return h_own.at[pl.ds(n * (share // 2), share // 2), :]

    def h_z(n):
        return rc(own_rows(n), h_rows(grp, n), HP, rh.at[grp * 2 + n], mate * 2 + y, t)

    def h_x(k, n):
        dest = lax.rem(x + k, nth) * 2 + c
        return rc(own_rows(n), h_rows(grp, n), HP, rh.at[grp * 2 + n], s, dest)

    def h_s0(n):
        return rc(own_rows(n), h_rows(grp, n), HS, one.at[HS], s, sib_t)

    def h_fwd(zz, k, n, far=False):
        g = zz * nth + lax.rem(x + nth - k, nth)
        ref = h_rows(g, n)
        arrived(ref, rh.at[g * 2 + n])
        if far:
            for i in range(1, nth):
                rc(ref, ref, HP, rh.at[g * 2 + n], s, lax.rem(x + i, nth) * 2 + c).start()
        rc(ref, ref, HS, one.at[HS], s, sib_t).start()

    def sib_c(n):
        return rc(sib_snd.at[n], sib_buf.at[n], SIB, rsib.at[n], s, sib_t)

    def red_c(n, k):
        g = lax.rem(grp + k, ng)
        sp, tp = grp_dev(g)
        return rc(red_snd.at[n, g], red_buf.at[n, grp], RED, rred.at[n], sp, tp)

    def other(q, m):
        r = lax.rem(zh + q, npair)
        return r * 2 + jnp.where(r > zh, m, 1 - m)

    def shared(zz):
        return (zz > z) == (mate > z)

    inner = jnp.logical_not(shared(other(1, 0))) if npair > 1 else z < 0

    def others(fn):
        for m in range(2):
            each(1, npair, lambda q: fn(other(q, m)))

    barrier = pltpu.get_barrier_semaphore()

    def greet(sp, tp):
        pl.semaphore_signal(barrier, inc=1, device_id={"sp": sp, "tp": tp}, device_id_type=MESH)

    for o in range(4 * ntp):
        sp, tt = zh * 4 + o // ntp, o % ntp
        pl.when((sp != s) | (tt != t))(functools.partial(greet, sp, tt))

    def greet_far(q):
        for o in range(8):
            greet(lax.rem(zh + q, npair) * 4 + o // 2, x * 2 + o % 2)

    each(1, npair, greet_far)
    for ld in qk_loads + v_loads + [lam_load]:
        ld.start()

    for ld in qk_loads + [lam_load]:
        ld.wait()
    for j in range(heads):
        at = slice(j * qk, (j + 1) * qk)
        qsl[j] = jnp.concatenate([qin[0, :, at], qin[1, :, at]], axis=1)
        slab[j, :, :qw] = jnp.concatenate([kin[0, :, at], kin[1, :, at]], axis=1)
        lam_all[c, j] = jnp.full(lam_all.shape[2:], lam_in[0, j], F32)
    for ld in v_loads:
        ld.wait()
    pl.semaphore_wait(barrier, 4 * ntp - 1 + 8 * (npair - 1))

    for j in range(heads):
        pl.when(jnp.logical_not(to_self(j)))(lambda: q_c(j).start())
    kv_out(lambda cp: cp.start(), True)
    kv_out(lambda cp: cp.start(), False)
    for j in range(heads):
        @pl.when(to_self(j))
        def _():
            q_buf[zl] = qsl[j]
            kv_buf[s] = slab[j]

    lam_c().start()
    each(1, nth, lambda k: ow_x(k).start())
    each(1, ntp, lambda k: st_c(k).start())
    ow_s0().start()
    def up_far(p):
        each(1, npair, lambda q: up_z(other(q, 1), p).start())
        each(1, npair, lambda q: up_z(other(q, 0), p).start())

    for p in range(2):
        up_y0(p).start()
    for p in range(2):
        up_z(mate, p).start()
    up_far(0)
    pl.when(inner)(lambda: up_far(1))
    for p in range(pieces):
        dn_y0(p).start()
    for ld in gain_loads + [st_load, ow_load, up_load, dn_load]:
        ld.start()

    m_run[...] = jnp.full(m_run.shape, -1e30, F32)
    l_run[...] = jnp.zeros(l_run.shape, F32)
    acc[...] = jnp.zeros(acc.shape, F32)
    scale = qk ** (-0.5)
    lane = lax.broadcasted_iota(jnp.int32, (tok, qw), 1)
    for i in range(2):
        pl.when(jnp.logical_not(self_worker & (zl == i)))(lambda: arrived(q_buf.at[i], rq.at[i]))
        qv = q_buf[i].astype(F32) * scale
        for mp in range(2):
            keep = (lane >= mp * qk) & (lane < (mp + 1) * qk)
            qm[mp, i * tok : (i + 1) * tok, :] = jnp.where(keep, qv, 0.0).astype(BF16)

    def absorb(block):
        v = block[:, qw:]
        for r in range(2):
            sc = lax.dot_general(block[:, :qw], qm[r], NT, preferred_element_type=F32)
            old = m_run[r]
            new = jnp.maximum(old, jnp.max(sc, axis=0, keepdims=True))
            fac = jnp.exp(old - new)
            ex = jnp.exp(sc - new)
            l_run[r] = l_run[r] * fac + jnp.sum(ex, axis=0, keepdims=True)
            acc[r] = acc[r] * fac + lax.dot_general(
                v, ex.astype(BF16), TN, preferred_element_type=F32
            )
            m_run[r] = new

    def step(i, carry):
        zz = lax.rem(zh * 2 + i // 2, nz)
        own = lax.rem(i, 2) == 0

        @pl.when(own)
        def _():
            direct = kv_buf.at[zz * 2 + c]
            pl.when(jnp.logical_not(self_worker & (zz == z)))(lambda: arrived(direct, rkv.at[zz]))
            kv_s(zz).start()

        pl.when(jnp.logical_not(own))(lambda: arrived(kv_buf.at[zz * 2 + 1 - c], rkvs.at[zz]))
        absorb(kv_buf.at[zz * 2 + jnp.where(own, c, 1 - c)])
        return carry

    lax.fori_loop(0, nsp, step, 0)

    for ld in gain_loads:
        ld.wait()
    arrived(lam_all.at[c], one.at[LAM])
    lam = lam_all[zl, y][:, :1]
    mixed = acc[0] / l_run[0] - lam * (acc[1] / l_run[1])
    inv = lax.rsqrt(jnp.mean(jnp.square(mixed), axis=0, keepdims=True) + 1e-05)
    normed = jnp.transpose(mixed * inv) * hg[...] * 0.8
    at_snd[...] = normed.astype(BF16)
    spots = [(i, tt) for i in range(2) for tt in range(ntp)]

    def at_mine(i, tt):
        return (i == zl) & (y == c) & (tt == t)

    for i, tt in spots:
        pl.when(jnp.logical_not(at_mine(i, tt)))(lambda: at_c(i, tt).start())

        @pl.when(at_mine(i, tt))
        def _():
            n = (i * ntp + tt) * share
            at_buf[head_t, :, at_cols()] = at_snd[n : n + share, :]

    def others_fwd(p):
        each(1, npair, lambda q: [up_fwd(other(q, m), p) for m in range(2)])

    pl.when(jnp.logical_not(inner))(lambda: up_far(1))
    for p in range(2):
        up_fwd(mate, p)
    for k in range(1, nth):
        ow_fwd(k)
    others_fwd(0)
    st_load.wait()
    arrived(st_buf.at[pl.ds(0, ntp - 1)], one.at[ST])
    cols = st_ref.shape[1]
    for b in range(ntp):
        pre[:, b * cols : (b + 1) * cols] = ALPHA * st_buf[b].astype(F32)
    at_all(lambda ref: arrived(ref, one.at[AT]))
    ow_load.wait()
    arrived(ow_buf.at[pl.ds(0, nth)], one.at[OW])
    for b in range(ntp):
        at = slice(b * cols, (b + 1) * cols)
        tot = pre[:, at]
        for tt in range(ntp):
            tot += jnp.dot(at_buf[tt], ow_buf[tt, :, at], preferred_element_type=F32)
        pre[:, at] = tot
    h_own[...] = layer_norm(pre[...], g1[...]).astype(BF16)
    for n in range(2):
        h_z(n).start()
        for k in range(1, nth):
            h_x(k, n).start()
        h_s0(n).start()
    for p in range(pieces):
        dn_z(mate, p).start()
    for p in range(pieces):
        each(1, npair, lambda q: dn_z(other(q, 0), p).start())
    h_buf[c, grp] = h_own[...]
    others_fwd(1)

    for n in range(2):
        h_fwd(1 - zl, 0, n, True)
    for p in range(pieces):
        each(1, npair, lambda q: dn_z(other(q, 1), p).start())
    for zz in (zl, 1 - zl):
        for n in range(2):
            for k in range(1, nth):
                h_fwd(zz, k, n)
    up_load.wait()
    arrived(up_buf.at[pl.ds(0, nz)], one.at[UP])
    arrived(h_buf.at[0], one.at[HS])

    half = ng * share
    for side in range(2):
        parts = 2 if fh % 256 == 0 else 1
        for n in range(parts):
            wide = fh // parts
            at = slice(n * wide, (n + 1) * wide)
            hid = h_buf[side].reshape(half, d)
            w = up_buf[:, :, at].reshape(d, wide)
            up = jnp.dot(hid, w, preferred_element_type=F32)
            act[side, :, at] = jnp.square(jnp.maximum(up, 0.0)).astype(BF16)
    dn_load.wait()

    steps = nz * pieces

    def unit(i):
        r = lax.rem(i, 2 * pieces)
        far = other(i // (2 * pieces), lax.rem(r, 2))
        zz = jnp.where(i < pieces, z, jnp.where(i < 2 * pieces, mate, far))
        return zz, jnp.where(i < 2 * pieces, lax.rem(i, pieces), r // 2)

    def index(i):
        zz, p = unit(i)
        return zz * pieces + p

    def finish(n):
        arrived(sib_buf.at[n], rsib.at[n])
        for k in range(ng - 1, 0, -1):
            g = lax.rem(grp + k, ng)
            rows = pl.ds(pl.multiple_of(g * share, share), share)
            red_snd[n, g] = (part[n, :, rows, :] + sib_buf[n, :, rows, :].astype(F32)).astype(BF16)
            red_c(n, k).start()
        rows = pl.ds(pl.multiple_of(grp * share, share), share)
        own_part[n] = part[n, :, rows, :] + sib_buf[n, :, rows, :].astype(F32)

    ahead, lead = pieces, 2

    def down(i, carry):
        pl.when((i + lead >= ahead) & (i + lead < steps))(lambda: dn_fwd(*unit(i + lead)))
        pl.when(i > 0)(lambda: finish(index(i - 1)))
        zz, p = unit(i)
        n = zz * pieces + p
        arrived(dn_buf.at[zz * 2 + 1 - y, :, cols_of(p)], rdy.at[n])
        at = cols_of(p)
        for yy in range(2):
            res = jnp.dot(act[1 - c], dn_buf[zz * 2 + yy, :, at], preferred_element_type=F32)
            sib_snd[n, yy] = res.astype(BF16)
        sib_c(n).start()
        for yy in range(2):
            part[n, yy] = jnp.dot(act[c], dn_buf[zz * 2 + yy, :, at], preferred_element_type=F32)
        return carry

    lax.fori_loop(0, steps, down, 0)
    finish(index(steps - 1))

    for zz in range(nz):
        for p in range(pieces):
            n = zz * pieces + p
            arrived(red_buf.at[n, pl.ds(0, ng - 1)], rred.at[n])
            for yy in range(2):
                lo = (zz * 2 + yy) * out_w + p * pw
                at = slice(lo, lo + pw)
                tot = own_part[n, yy] + ALPHA * h_own[:, at].astype(F32)
                for k in range(ng - 1, 0, -1):
                    tot += red_buf[n, lax.rem(grp + ng - k, ng), yy].astype(F32)
                pre[:, at] = tot
    out_ref[...] = layer_norm(pre[...], g2[...]).astype(BF16)

    for kind, buf, most in ((Q, qsl, heads), (KV, kv_buf, npair * heads)):
        pl.when(self_worker)(lambda: left(buf.at[pl.ds(0, most - 1)], kind))
        pl.when(jnp.logical_not(self_worker))(lambda: left(buf.at[pl.ds(0, most)], kind))
    at_all(lambda ref: left(ref, AT))
    left(lam_all.at[c], LAM)
    left(kv_buf.at[pl.ds(0, nz)], KVS)
    left(up_buf.at[pl.ds(0, nsp - 1)], UP)
    left(dn_buf.at[pl.ds(0, nsp - 1)], DN)
    left(ow_buf.at[pl.ds(0, ntp - 1)], OW)
    left(st_buf.at[pl.ds(0, ntp - 1)], ST)
    left(h_buf.at[0, pl.ds(0, ng - 1)], HP)
    left(h_buf.at[0], HS)
    left(sib_snd, SIB)
    left(red_snd.at[:, pl.ds(0, ng - 1)], RED)


def local(nsp, ntp, q1, q2, k1, k2, vals, lam, hg, stream, ow, g1, up, dn, g2):
    tok = q1.shape[0]
    heads = lam.shape[0]
    hv = vals.shape[1]
    vd = hv // heads
    d = ow.shape[1]
    nz, nth = nsp // 2, ntp // 2
    ng = 2 * nth
    share = tok // ntp
    fh = up.shape[1] // 2
    qk = q1.shape[1] // heads
    half, out_w = ng * share, dn.shape[1]
    pieces = 2 if out_w % 256 == 0 else 1
    units, pw = nz * pieces, out_w // pieces
    vm = pl.BlockSpec(memory_space=pltpu.VMEM)
    hbm = pl.BlockSpec(memory_space=pl.ANY)
    sems = (KINDS, KINDS, 2, nz, nz, 2 * nz, units, units, nth, 2 * ng, units, units)
    return pl.pallas_call(
        functools.partial(kernel, nsp, ntp, heads, pieces),
        out_shape=pltpu.VMEM((share, d), BF16),
        in_specs=[hbm] * 13,
        out_specs=vm,
        scratch_shapes=[
            pltpu.SMEM((1, heads), F32),
            pltpu.VMEM((2, heads, 1, 128), F32),
            pltpu.VMEM((2, tok, heads * qk), BF16),
            pltpu.VMEM((2, tok, heads * qk), BF16),
            pltpu.VMEM((heads, tok, 2 * qk), BF16),
            pltpu.VMEM((heads, tok, 2 * qk + vd), BF16),
            pltpu.VMEM((1, vd), F32),
            pltpu.VMEM((1, d), F32),
            pltpu.VMEM((1, d), F32),
            pltpu.VMEM((2, tok, 2 * qk), BF16),
            pltpu.VMEM((2, 2 * tok, 2 * qk), BF16),
            pltpu.VMEM((2, 1, 2 * tok), F32),
            pltpu.VMEM((2, 1, 2 * tok), F32),
            pltpu.VMEM((2, vd, 2 * tok), F32),
            pltpu.VMEM((nsp, tok, 2 * qk + vd), BF16),
            pltpu.VMEM((nsp, up.shape[0], fh), BF16),
            pltpu.VMEM((nsp, fh, out_w), BF16),
            pltpu.VMEM((ntp,) + ow.shape, BF16),
            pltpu.VMEM((ntp, share, stream.shape[1]), BF16),
            pltpu.VMEM((2 * tok, vd), BF16),
            pltpu.VMEM((ntp, share, hv), BF16),
            pltpu.VMEM((share, d), F32),
            pltpu.VMEM((share, d), BF16),
            pltpu.VMEM((2, ng, share, d), BF16),
            pltpu.VMEM((2, half, fh), BF16),
            pltpu.VMEM((units, 2, half, pw), BF16),
            pltpu.VMEM((units, 2, half, pw), BF16),
            pltpu.VMEM((units, 2, half, pw), F32),
            pltpu.VMEM((units, 2, share, pw), F32),
            pltpu.VMEM((units, ng, 2, share, pw), BF16),
            pltpu.VMEM((units, ng, 2, share, pw), BF16),
            pltpu.SemaphoreType.DMA((5 + heads + 7,)),
            *[pltpu.SemaphoreType.DMA((n,)) for n in sems],
        ],
        compiler_params=pltpu.CompilerParams(
            collective_id=0, has_side_effects=True, vmem_limit_bytes=60 * 1024 * 1024
        ),
    )(
        lam.reshape(1, heads), q1, q2, k1, k2, vals, hg.reshape(1, vd), stream, ow,
        g1.reshape(1, d), up, dn, g2.reshape(1, d),
    )


def solution(mesh):
    in_specs = (
        P("sp", "tp"),
        P("sp", "tp"),
        P("sp", "tp"),
        P("sp", "tp"),
        P("sp", "tp"),
        P("tp"),
        P(),
        P("sp", "tp"),
        P("tp", None),
        P(),
        P("sp", "tp"),
        P("tp", "sp"),
        P(),
    )
    body = functools.partial(local, mesh.shape["sp"], mesh.shape["tp"])
    return jax.shard_map(
        body, mesh=mesh, in_specs=in_specs, out_specs=P(("sp", "tp"), None), check_vma=False
    )
```

```python
import functools

import jax
import jax.numpy as jnp
from jax import lax
from jax.experimental import pallas as pl
from jax.experimental.pallas import tpu as pltpu
from jax.sharding import PartitionSpec as P

MESH = pl.DeviceIdType.MESH
F32, BF16 = jnp.float32, jnp.bfloat16
ALPHA = 2.0**0.5
NT = (((1,), (1,)), ((), ()))
TN = (((0,), (0,)), ((), ()))
KINDS = 13
SHARED = 6
LAM, UP, OW, ST, AT, HS, Q, KV, KVS, DN, HP, SIB, RED = range(KINDS)


def layer_norm(value, gain):
    centre = jnp.mean(value, axis=-1, keepdims=True)
    spread = jnp.mean(jnp.square(value - centre), axis=-1, keepdims=True)
    return (value - centre) * lax.rsqrt(spread + 1e-05) * gain


def kernel(
    nsp, ntp, heads, pieces,
    lam_ref, q1_ref, q2_ref, k1_ref, k2_ref, v_ref, hg_ref, st_ref, ow_ref, g1_ref, up_ref, dn_ref, g2_ref,
    out_ref,
    lam_in, lam_all, qin, kin, qsl, slab, hg, g1, g2,
    q_buf, qm, m_run, l_run, acc, kv_buf, up_buf, dn_buf, ow_buf, st_buf, at_snd, at_buf,
    pre, h_own, h_buf, act, sib_snd, sib_buf, part, own_part, red_snd, red_buf,
    loc_sem, snd, one, rq, rkv, rkvs, rup, rdz, rdy, rox, rh, rsib, rred,
):
    s, t = lax.axis_index("sp"), lax.axis_index("tp")
    nz, nth = nsp // 2, ntp // 2
    npair = nz // 2
    ng = 2 * nth
    z, y = s // 2, s % 2
    zh, zl = z // 2, z % 2
    mate = zh * 2 + 1 - zl
    x, c = t // 2, t % 2
    sib_t = x * 2 + (1 - c)
    y_sp = z * 2 + (1 - y)
    grp = zl * nth + x
    tok = q1_ref.shape[0]
    share = tok // ntp
    fh = up_ref.shape[1] // 2
    vd = acc.shape[1]
    qw = q_buf.shape[2]
    qk = qw // 2
    d = pre.shape[1]
    out_w = dn_buf.shape[2]
    pw = out_w // pieces
    head_t = x * 2 + zl

    def rc(src, dst, kind, arrive, sp, tp):
        return pltpu.make_async_remote_copy(
            src_ref=src, dst_ref=dst, send_sem=snd.at[kind], recv_sem=arrive,
            device_id={"sp": sp, "tp": tp}, device_id_type=MESH,
        )

    def arrived(ref, sem):
        rc(ref, ref, 0, sem, y_sp, t).wait_recv()

    def left(ref, kind):
        rc(ref, ref, kind, one.at[LAM], y_sp, t).wait_send()

    def each(lo, hi, body):
        if hi - lo <= 4:
            for k in range(lo, hi):
                body(k)
        else:
            lax.fori_loop(lo, hi, lambda k, carry: (body(k), carry)[1], 0)

    def lc(src, dst, i):
        return pltpu.make_async_copy(src, dst, loc_sem.at[i])

    def up_half(j):
        return up_ref.at[:, pl.ds(pl.multiple_of(j * fh, fh), fh)]

    def dn_rows(j):
        return pl.ds(pl.multiple_of(j * fh, fh), fh)

    def rows_of(tt):
        return pl.ds(pl.multiple_of(tt * share, share), share)

    qk_loads = [
        lc(q1_ref, qin.at[0], 0),
        lc(q2_ref, qin.at[1], 1),
        lc(k1_ref, kin.at[0], 2),
        lc(k2_ref, kin.at[1], 3),
    ]
    v_loads = [
        lc(v_ref.at[:, pl.ds(j * vd, vd)], slab.at[j, :, pl.ds(qw, vd)], 4 + j) for j in range(heads)
    ]
    n0 = 5 + heads
    lam_load = lc(lam_ref, lam_in, 4 + heads)
    gain_loads = [lc(hg_ref, hg, n0), lc(g1_ref, g1, n0 + 1), lc(g2_ref, g2, n0 + 2)]
    up_load = lc(up_half(zl), up_buf.at[s], n0 + 3)
    dn_load = lc(dn_ref.at[dn_rows(zl), :], dn_buf.at[s], n0 + 4)
    ow_load = lc(ow_ref, ow_buf.at[t], n0 + 5)
    st_load = lc(st_ref.at[rows_of(t), :], st_buf.at[t], n0 + 6)

    def lam_c():
        return rc(lam_all.at[c], lam_all.at[c], LAM, one.at[LAM], s, sib_t)

    def to_self(j):
        return (c == zl) & (y == c) & (j == y)

    self_worker = (c == zl) & (y == c)

    def q_c(j):
        return rc(qsl.at[j], q_buf.at[zl], Q, rq.at[zl], (zh * 2 + c) * 2 + j, x * 2 + y)

    def kv_c(r, j):
        return rc(slab.at[j], kv_buf.at[s], KV, rkv.at[z], (r * 2 + c) * 2 + j, x * 2 + y)

    def kv_s(zz):
        ref = kv_buf.at[zz * 2 + c]
        return rc(ref, ref, KVS, rkvs.at[zz], s, sib_t)

    def kv_out(fn, own):
        for j in range(heads):
            if own:
                pl.when(jnp.logical_not(to_self(j)))(lambda: fn(kv_c(zh, j)))
            else:
                each(1, npair, lambda q: fn(kv_c(lax.rem(zh + q, npair), j)))

    ur = up_ref.shape[0] // 2

    def up_rows(p):
        return pl.ds(p * ur, ur)

    def up_part(j, p):
        return up_ref.at[up_rows(p), pl.ds(pl.multiple_of(j * fh, fh), fh)]

    def up_z(zz, p):
        return rc(up_part(zz % 2, p), up_buf.at[s, up_rows(p)], UP, rup.at[z * 2 + p], zz * 2 + y, t)

    def up_y0(p):
        return rc(up_part(zl, p), up_buf.at[s, up_rows(p)], UP, one.at[UP], y_sp, t)

    def up_fwd(zz, p):
        ref = up_buf.at[zz * 2 + y, up_rows(p)]
        arrived(ref, rup.at[zz * 2 + p])
        rc(ref, ref, UP, one.at[UP], y_sp, t).start()

    def cols_of(p):
        if pieces == 1:
            return pl.ds(0, pw)
        return pl.ds(p * pw if isinstance(p, int) else pl.multiple_of(p * pw, pw), pw)

    def dn_part(j, p):
        return dn_ref.at[dn_rows(j), cols_of(p)]

    def dn_z(zz, p):
        return rc(
            dn_part(zz % 2, p), dn_buf.at[s, :, cols_of(p)], DN, rdz.at[z * pieces + p], zz * 2 + y, t
        )

    def dn_y0(p):
        return rc(dn_part(zl, p), dn_buf.at[s, :, cols_of(p)], DN, rdy.at[z * pieces + p], y_sp, t)

    def dn_fwd(zz, p):
        ref = dn_buf.at[zz * 2 + y, :, cols_of(p)]
        arrived(ref, rdz.at[zz * pieces + p])
        rc(ref, ref, DN, rdy.at[zz * pieces + p], y_sp, t).start()

    def ow_x(k):
        return rc(ow_ref, ow_buf.at[t], OW, rox.at[k], s, lax.rem(x + k, nth) * 2 + c)

    def ow_s0():
        return rc(ow_ref, ow_buf.at[t], OW, one.at[OW], s, sib_t)

    def ow_fwd(k):
        ref = ow_buf.at[lax.rem(x + nth - k, nth) * 2 + c]
        arrived(ref, rox.at[k])
        rc(ref, ref, OW, one.at[OW], s, sib_t).start()

    def st_c(k):
        td = lax.rem(t + k, ntp)
        return rc(st_ref.at[rows_of(td), :], st_buf.at[t], ST, one.at[ST], s, td)

    def at_cols():
        return pl.ds(pl.multiple_of(y * vd, vd), vd)

    def at_c(i, tt):
        rows = pl.ds((i * ntp + tt) * share, share)
        return rc(
            at_snd.at[rows, :], at_buf.at[head_t, :, at_cols()], AT, one.at[AT], (zh * 2 + i) * 2 + c, tt
        )

    def at_all(fn):
        pl.when(y == c)(lambda: fn(at_snd.at[pl.ds(0, 2 * tok - share)]))
        pl.when(y != c)(lambda: fn(at_snd.at[pl.ds(0, 2 * tok)]))

    def grp_dev(g):
        return (zh * 2 + g // nth) * 2 + y, lax.rem(g, nth) * 2 + c

    def h_rows(g, n):
        return h_buf.at[c, g, pl.ds(n * (share // 2), share // 2), :]

    def own_rows(n):
        return h_own.at[pl.ds(n * (share // 2), share // 2), :]

    def h_z(n):
        return rc(own_rows(n), h_rows(grp, n), HP, rh.at[grp * 2 + n], mate * 2 + y, t)

    def h_x(k, n):
        dest = lax.rem(x + k, nth) * 2 + c
        return rc(own_rows(n), h_rows(grp, n), HP, rh.at[grp * 2 + n], s, dest)

    def h_s0(n):
        return rc(own_rows(n), h_rows(grp, n), HS, one.at[HS], s, sib_t)

    def h_fwd(zz, k, n, far=False):
        g = zz * nth + lax.rem(x + nth - k, nth)
        ref = h_rows(g, n)
        arrived(ref, rh.at[g * 2 + n])
        if far:
            for i in range(1, nth):
                rc(ref, ref, HP, rh.at[g * 2 + n], s, lax.rem(x + i, nth) * 2 + c).start()
        rc(ref, ref, HS, one.at[HS], s, sib_t).start()

    def red_c(n, k):
        g = lax.rem(grp + k, ng)
        sp, tp = grp_dev(g)
        return rc(red_snd.at[n, g], red_buf.at[n, grp], RED, rred.at[n], sp, tp)

    def other(q, m):
        r = lax.rem(zh + q, npair)
        return r * 2 + jnp.where(r > zh, m, 1 - m)

    def shared(zz):
        return (zz > z) == (mate > z)

    inner = jnp.logical_not(shared(other(1, 0))) if npair > 1 else z < 0

    def others(fn):
        for m in range(2):
            each(1, npair, lambda q: fn(other(q, m)))

    barrier = pltpu.get_barrier_semaphore()

    def greet(sp, tp):
        pl.semaphore_signal(barrier, inc=1, device_id={"sp": sp, "tp": tp}, device_id_type=MESH)

    for o in range(4 * ntp):
        sp, tt = zh * 4 + o // ntp, o % ntp
        pl.when((sp != s) | (tt != t))(functools.partial(greet, sp, tt))

    def greet_far(q):
        for o in range(8):
            greet(lax.rem(zh + q, npair) * 4 + o // 2, x * 2 + o % 2)

    each(1, npair, greet_far)
    for ld in qk_loads + v_loads + [lam_load]:
        ld.start()

    for ld in qk_loads + [lam_load]:
        ld.wait()
    for j in range(heads):
        at = slice(j * qk, (j + 1) * qk)
        qsl[j] = jnp.concatenate([qin[0, :, at], qin[1, :, at]], axis=1)
        slab[j, :, :qw] = jnp.concatenate([kin[0, :, at], kin[1, :, at]], axis=1)
        lam_all[c, j] = jnp.full(lam_all.shape[2:], lam_in[0, j], F32)
    for ld in v_loads:
        ld.wait()
    pl.semaphore_wait(barrier, 4 * ntp - 1 + 8 * (npair - 1))

    for j in range(heads):
        pl.when(jnp.logical_not(to_self(j)))(lambda: q_c(j).start())
    kv_out(lambda cp: cp.start(), True)
    kv_out(lambda cp: cp.start(), False)
    for j in range(heads):
        @pl.when(to_self(j))
        def _():
            q_buf[zl] = qsl[j]
            kv_buf[s] = slab[j]

    lam_c().start()
    each(1, nth, lambda k: ow_x(k).start())
    each(1, ntp, lambda k: st_c(k).start())
    ow_s0().start()
    def up_far(p):
        each(1, npair, lambda q: up_z(other(q, 1), p).start())
        each(1, npair, lambda q: up_z(other(q, 0), p).start())

    for p in range(2):
        up_y0(p).start()
    for p in range(2):
        up_z(mate, p).start()
    up_far(0)
    pl.when(inner)(lambda: up_far(1))
    for p in range(pieces):
        dn_y0(p).start()
    for ld in gain_loads + [st_load, ow_load, up_load, dn_load]:
        ld.start()

    m_run[...] = jnp.full(m_run.shape, -1e30, F32)
    l_run[...] = jnp.zeros(l_run.shape, F32)
    acc[...] = jnp.zeros(acc.shape, F32)
    scale = qk ** (-0.5)
    lane = lax.broadcasted_iota(jnp.int32, (tok, qw), 1)
    for i in range(2):
        pl.when(jnp.logical_not(self_worker & (zl == i)))(lambda: arrived(q_buf.at[i], rq.at[i]))
        qv = q_buf[i].astype(F32) * scale
        for mp in range(2):
            keep = (lane >= mp * qk) & (lane < (mp + 1) * qk)
            qm[mp, i * tok : (i + 1) * tok, :] = jnp.where(keep, qv, 0.0).astype(BF16)

    def absorb(block):
        v = block[:, qw:]
        for r in range(2):
            sc = lax.dot_general(block[:, :qw], qm[r], NT, preferred_element_type=F32)
            old = m_run[r]
            new = jnp.maximum(old, jnp.max(sc, axis=0, keepdims=True))
            fac = jnp.exp(old - new)
            ex = jnp.exp(sc - new)
            l_run[r] = l_run[r] * fac + jnp.sum(ex, axis=0, keepdims=True)
            acc[r] = acc[r] * fac + lax.dot_general(
                v, ex.astype(BF16), TN, preferred_element_type=F32
            )
            m_run[r] = new

    def step(i, carry):
        zz = lax.rem(zh * 2 + i // 2, nz)
        own = lax.rem(i, 2) == 0

        @pl.when(own)
        def _():
            direct = kv_buf.at[zz * 2 + c]
            pl.when(jnp.logical_not(self_worker & (zz == z)))(lambda: arrived(direct, rkv.at[zz]))
            kv_s(zz).start()

        pl.when(jnp.logical_not(own))(lambda: arrived(kv_buf.at[zz * 2 + 1 - c], rkvs.at[zz]))
        absorb(kv_buf.at[zz * 2 + jnp.where(own, c, 1 - c)])
        return carry

    lax.fori_loop(0, nsp, step, 0)

    for ld in gain_loads:
        ld.wait()
    arrived(lam_all.at[c], one.at[LAM])
    lam = lam_all[zl, y][:, :1]
    mixed = acc[0] / l_run[0] - lam * (acc[1] / l_run[1])
    inv = lax.rsqrt(jnp.mean(jnp.square(mixed), axis=0, keepdims=True) + 1e-05)
    normed = jnp.transpose(mixed * inv) * hg[...] * 0.8
    at_snd[...] = normed.astype(BF16)
    spots = [(i, tt) for i in range(2) for tt in range(ntp)]

    def at_mine(i, tt):
        return (i == zl) & (y == c) & (tt == t)

    for i, tt in spots:
        pl.when(jnp.logical_not(at_mine(i, tt)))(lambda: at_c(i, tt).start())

        @pl.when(at_mine(i, tt))
        def _():
            n = (i * ntp + tt) * share
            at_buf[head_t, :, at_cols()] = at_snd[n : n + share, :]

    def others_fwd(p):
        each(1, npair, lambda q: [up_fwd(other(q, m), p) for m in range(2)])

    pl.when(jnp.logical_not(inner))(lambda: up_far(1))
    for p in range(2):
        up_fwd(mate, p)
    for k in range(1, nth):
        ow_fwd(k)
    others_fwd(0)
    st_load.wait()
    arrived(st_buf.at[pl.ds(0, ntp - 1)], one.at[ST])
    cols = st_ref.shape[1]
    for b in range(ntp):
        pre[:, b * cols : (b + 1) * cols] = ALPHA * st_buf[b].astype(F32)
    at_all(lambda ref: arrived(ref, one.at[AT]))
    ow_load.wait()
    arrived(ow_buf.at[pl.ds(0, nth)], one.at[OW])
    for b in range(ntp):
        at = slice(b * cols, (b + 1) * cols)
        tot = pre[:, at]
        for tt in range(ntp):
            tot += jnp.dot(at_buf[tt], ow_buf[tt, :, at], preferred_element_type=F32)
        pre[:, at] = tot
    h_own[...] = layer_norm(pre[...], g1[...]).astype(BF16)
    for n in range(2):
        h_z(n).start()
        for k in range(1, nth):
            h_x(k, n).start()
        h_s0(n).start()
    for p in range(pieces):
        dn_z(mate, p).start()
    for p in range(pieces):
        each(1, npair, lambda q: dn_z(other(q, 0), p).start())
    h_buf[c, grp] = h_own[...]
    others_fwd(1)

    for n in range(2):
        h_fwd(1 - zl, 0, n, True)
    for p in range(pieces):
        each(1, npair, lambda q: dn_z(other(q, 1), p).start())
    for zz in (zl, 1 - zl):
        for n in range(2):
            for k in range(1, nth):
                h_fwd(zz, k, n)
    up_load.wait()
    arrived(up_buf.at[pl.ds(0, nz)], one.at[UP])
    arrived(h_buf.at[0], one.at[HS])

    half = ng * share
    for side in range(2):
        parts = 2 if fh % 256 == 0 else 1
        for n in range(parts):
            wide = fh // parts
            at = slice(n * wide, (n + 1) * wide)
            hid = h_buf[side].reshape(half, d)
            w = up_buf[:, :, at].reshape(d, wide)
            up = jnp.dot(hid, w, preferred_element_type=F32)
            act[side, :, at] = jnp.square(jnp.maximum(up, 0.0)).astype(BF16)
    dn_load.wait()

    steps = nz * pieces

    def unit(i):
        r = lax.rem(i, 2 * pieces)
        far = other(i // (2 * pieces), lax.rem(r, 2))
        zz = jnp.where(i < pieces, z, jnp.where(i < 2 * pieces, mate, far))
        return zz, jnp.where(i < 2 * pieces, lax.rem(i, pieces), r // 2)

    def index(i):
        zz, p = unit(i)
        return zz * pieces + p

    def finish(n):
        arrived(sib_buf.at[n], rsib.at[n])
        for k in range(ng - 1, 0, -1):
            g = lax.rem(grp + k, ng)
            rows = pl.ds(pl.multiple_of(g * share, share), share)
            red_snd[n, g] = (part[n, :, rows, :] + sib_buf[n, :, rows, :].astype(F32)).astype(BF16)
            red_c(n, k).start()
        rows = pl.ds(pl.multiple_of(grp * share, share), share)
        own_part[n] = part[n, :, rows, :] + sib_buf[n, :, rows, :].astype(F32)

    ahead, lead = pieces, 2

    def down(i, carry):
        pl.when((i + lead >= ahead) & (i + lead < steps))(lambda: dn_fwd(*unit(i + lead)))
        pl.when(i > 0)(lambda: finish(index(i - 1)))
        zz, p = unit(i)
        n = zz * pieces + p
        arrived(dn_buf.at[zz * 2 + 1 - y, :, cols_of(p)], rdy.at[n])
        at = cols_of(p)
        w = jnp.concatenate([dn_buf[zz * 2, :, at], dn_buf[zz * 2 + 1, :, at]], axis=1)
        res = jnp.dot(act[1 - c], w, preferred_element_type=F32)
        for yy in range(2):
            sib_snd[n, yy] = res[:, yy * pw : (yy + 1) * pw].astype(BF16)
            rc(sib_snd.at[n, yy], sib_buf.at[n, yy], SIB, rsib.at[n], s, sib_t).start()
        res = jnp.dot(act[c], w, preferred_element_type=F32)
        for yy in range(2):
            part[n, yy] = res[:, yy * pw : (yy + 1) * pw]
        return carry

    lax.fori_loop(0, steps, down, 0)
    finish(index(steps - 1))

    for zz in range(nz):
        for p in range(pieces):
            n = zz * pieces + p
            arrived(red_buf.at[n, pl.ds(0, ng - 1)], rred.at[n])
            for yy in range(2):
                lo = (zz * 2 + yy) * out_w + p * pw
                at = slice(lo, lo + pw)
                tot = own_part[n, yy] + ALPHA * h_own[:, at].astype(F32)
                for k in range(ng - 1, 0, -1):
                    tot += red_buf[n, lax.rem(grp + ng - k, ng), yy].astype(F32)
                pre[:, at] = tot
    out_ref[...] = layer_norm(pre[...], g2[...]).astype(BF16)

    for kind, buf, most in ((Q, qsl, heads), (KV, kv_buf, npair * heads)):
        pl.when(self_worker)(lambda: left(buf.at[pl.ds(0, most - 1)], kind))
        pl.when(jnp.logical_not(self_worker))(lambda: left(buf.at[pl.ds(0, most)], kind))
    at_all(lambda ref: left(ref, AT))
    left(lam_all.at[c], LAM)
    left(kv_buf.at[pl.ds(0, nz)], KVS)
    left(up_buf.at[pl.ds(0, nsp - 1)], UP)
    left(dn_buf.at[pl.ds(0, nsp - 1)], DN)
    left(ow_buf.at[pl.ds(0, ntp - 1)], OW)
    left(st_buf.at[pl.ds(0, ntp - 1)], ST)
    left(h_buf.at[0, pl.ds(0, ng - 1)], HP)
    left(h_buf.at[0], HS)
    left(sib_snd, SIB)
    left(red_snd.at[:, pl.ds(0, ng - 1)], RED)


def local(nsp, ntp, q1, q2, k1, k2, vals, lam, hg, stream, ow, g1, up, dn, g2):
    tok = q1.shape[0]
    heads = lam.shape[0]
    hv = vals.shape[1]
    vd = hv // heads
    d = ow.shape[1]
    nz, nth = nsp // 2, ntp // 2
    ng = 2 * nth
    share = tok // ntp
    fh = up.shape[1] // 2
    qk = q1.shape[1] // heads
    half, out_w = ng * share, dn.shape[1]
    pieces = 2 if out_w % 256 == 0 else 1
    units, pw = nz * pieces, out_w // pieces
    vm = pl.BlockSpec(memory_space=pltpu.VMEM)
    hbm = pl.BlockSpec(memory_space=pl.ANY)
    sems = (KINDS, SHARED, 2, nz, nz, 2 * nz, units, units, nth, 2 * ng, units, units)
    return pl.pallas_call(
        functools.partial(kernel, nsp, ntp, heads, pieces),
        out_shape=pltpu.VMEM((share, d), BF16),
        in_specs=[hbm] * 13,
        out_specs=vm,
        scratch_shapes=[
            pltpu.SMEM((1, heads), F32),
            pltpu.VMEM((2, heads, 1, 128), F32),
            pltpu.VMEM((2, tok, heads * qk), BF16),
            pltpu.VMEM((2, tok, heads * qk), BF16),
            pltpu.VMEM((heads, tok, 2 * qk), BF16),
            pltpu.VMEM((heads, tok, 2 * qk + vd), BF16),
            pltpu.VMEM((1, vd), F32),
            pltpu.VMEM((1, d), F32),
            pltpu.VMEM((1, d), F32),
            pltpu.VMEM((2, tok, 2 * qk), BF16),
            pltpu.VMEM((2, 2 * tok, 2 * qk), BF16),
            pltpu.VMEM((2, 1, 2 * tok), F32),
            pltpu.VMEM((2, 1, 2 * tok), F32),
            pltpu.VMEM((2, vd, 2 * tok), F32),
            pltpu.VMEM((nsp, tok, 2 * qk + vd), BF16),
            pltpu.VMEM((nsp, up.shape[0], fh), BF16),
            pltpu.VMEM((nsp, fh, out_w), BF16),
            pltpu.VMEM((ntp,) + ow.shape, BF16),
            pltpu.VMEM((ntp, share, stream.shape[1]), BF16),
            pltpu.VMEM((2 * tok, vd), BF16),
            pltpu.VMEM((ntp, share, hv), BF16),
            pltpu.VMEM((share, d), F32),
            pltpu.VMEM((share, d), BF16),
            pltpu.VMEM((2, ng, share, d), BF16),
            pltpu.VMEM((2, half, fh), BF16),
            pltpu.VMEM((units, 2, half, pw), BF16),
            pltpu.VMEM((units, 2, half, pw), BF16),
            pltpu.VMEM((units, 2, half, pw), F32),
            pltpu.VMEM((units, 2, share, pw), F32),
            pltpu.VMEM((units, ng, 2, share, pw), BF16),
            pltpu.VMEM((units, ng, 2, share, pw), BF16),
            pltpu.SemaphoreType.DMA((5 + heads + 7,)),
            *[pltpu.SemaphoreType.DMA((n,)) for n in sems],
        ],
        compiler_params=pltpu.CompilerParams(
            collective_id=0, has_side_effects=True, vmem_limit_bytes=60 * 1024 * 1024
        ),
    )(
        lam.reshape(1, heads), q1, q2, k1, k2, vals, hg.reshape(1, vd), stream, ow,
        g1.reshape(1, d), up, dn, g2.reshape(1, d),
    )


def solution(mesh):
    in_specs = (
        P("sp", "tp"),
        P("sp", "tp"),
        P("sp", "tp"),
        P("sp", "tp"),
        P("sp", "tp"),
        P("tp"),
        P(),
        P("sp", "tp"),
        P("tp", None),
        P(),
        P("sp", "tp"),
        P("tp", "sp"),
        P(),
    )
    body = functools.partial(local, mesh.shape["sp"], mesh.shape["tp"])
    return jax.shard_map(
        body, mesh=mesh, in_specs=in_specs, out_specs=P(("sp", "tp"), None), check_vma=False
    )
```

```python
import functools

import jax
import jax.numpy as jnp
from jax import lax
from jax.experimental import pallas as pl
from jax.experimental.pallas import tpu as pltpu
from jax.sharding import PartitionSpec as P

MESH = pl.DeviceIdType.MESH
F32, BF16 = jnp.float32, jnp.bfloat16
ALPHA = 2.0**0.5
NT = (((1,), (1,)), ((), ()))
TN = (((0,), (0,)), ((), ()))
KINDS = 13
LAM, Q, KV, KVS, UP, DN, OW, ST, AT, HP, HS, SIB, RED = range(KINDS)


def layer_norm(value, gain):
    centre = jnp.mean(value, axis=-1, keepdims=True)
    spread = jnp.mean(jnp.square(value - centre), axis=-1, keepdims=True)
    return (value - centre) * lax.rsqrt(spread + 1e-05) * gain


def kernel(
    nsp, ntp, heads, pieces,
    lam_ref, q1_ref, q2_ref, k1_ref, k2_ref, v_ref, hg_ref, st_ref, ow_ref, g1_ref, up_ref, dn_ref, g2_ref,
    out_ref,
    lam_in, lam_all, qin, kin, qsl, slab, hg, g1, g2,
    q_buf, qm, m_run, l_run, acc, kv_buf, up_buf, dn_buf, ow_buf, st_buf, at_snd, at_buf,
    pre, h_own, h_buf, act, sib_snd, sib_buf, part, own_part, red_snd, red_buf,
    loc_sem, snd, one, rq, rkv, rkvs, rup, rdz, rdy, rox, rh, rsib, rred,
):
    s, t = lax.axis_index("sp"), lax.axis_index("tp")
    nz, nth = nsp // 2, ntp // 2
    npair = nz // 2
    ng = 2 * nth
    z, y = s // 2, s % 2
    zh, zl = z // 2, z % 2
    mate = zh * 2 + 1 - zl
    x, c = t // 2, t % 2
    sib_t = x * 2 + (1 - c)
    y_sp = z * 2 + (1 - y)
    grp = zl * nth + x
    tok = q1_ref.shape[0]
    share = tok // ntp
    fh = up_ref.shape[1] // 2
    vd = acc.shape[1]
    qw = q_buf.shape[2]
    qk = qw // 2
    d = pre.shape[1]
    out_w = dn_buf.shape[2]
    pw = out_w // pieces
    head_t = x * 2 + zl

    def rc(src, dst, kind, arrive, sp, tp):
        return pltpu.make_async_remote_copy(
            src_ref=src, dst_ref=dst, send_sem=snd.at[kind], recv_sem=arrive,
            device_id={"sp": sp, "tp": tp}, device_id_type=MESH,
        )

    def arrived(ref, sem):
        rc(ref, ref, 0, sem, y_sp, t).wait_recv()

    def left(ref, kind):
        rc(ref, ref, kind, one.at[LAM], y_sp, t).wait_send()

    def each(lo, hi, body):
        if hi - lo <= 4:
            for k in range(lo, hi):
                body(k)
        else:
            lax.fori_loop(lo, hi, lambda k, carry: (body(k), carry)[1], 0)

    def lc(src, dst, i):
        return pltpu.make_async_copy(src, dst, loc_sem.at[i])

    def up_half(j):
        return up_ref.at[:, pl.ds(pl.multiple_of(j * fh, fh), fh)]

    def dn_rows(j):
        return pl.ds(pl.multiple_of(j * fh, fh), fh)

    def rows_of(tt):
        return pl.ds(pl.multiple_of(tt * share, share), share)

    qk_loads = [
        lc(q1_ref, qin.at[0], 0),
        lc(q2_ref, qin.at[1], 1),
        lc(k1_ref, kin.at[0], 2),
        lc(k2_ref, kin.at[1], 3),
    ]
    v_loads = [
        lc(v_ref.at[:, pl.ds(j * vd, vd)], slab.at[j, :, pl.ds(qw, vd)], 4 + j) for j in range(heads)
    ]
    n0 = 5 + heads
    lam_load = lc(lam_ref, lam_in, 4 + heads)
    gain_loads = [lc(hg_ref, hg, n0), lc(g1_ref, g1, n0 + 1), lc(g2_ref, g2, n0 + 2)]
    up_load = lc(up_half(zl), up_buf.at[s], n0 + 3)
    dn_load = lc(dn_ref.at[dn_rows(zl), :], dn_buf.at[s], n0 + 4)
    ow_load = lc(ow_ref, ow_buf.at[t], n0 + 5)
    st_load = lc(st_ref.at[rows_of(t), :], st_buf.at[t], n0 + 6)

    def lam_c():
        return rc(lam_all.at[c], lam_all.at[c], LAM, one.at[LAM], s, sib_t)

    def to_self(j):
        return (c == zl) & (y == c) & (j == y)

    self_worker = (c == zl) & (y == c)

    def q_c(j):
        return rc(qsl.at[j], q_buf.at[zl], Q, rq.at[zl], (zh * 2 + c) * 2 + j, x * 2 + y)

    def kv_c(r, j):
        return rc(slab.at[j], kv_buf.at[s], KV, rkv.at[z], (r * 2 + c) * 2 + j, x * 2 + y)

    def kv_s(zz):
        ref = kv_buf.at[zz * 2 + c]
        return rc(ref, ref, KVS, rkvs.at[zz], s, sib_t)

    def kv_out(fn, own):
        for j in range(heads):
            if own:
                pl.when(jnp.logical_not(to_self(j)))(lambda: fn(kv_c(zh, j)))
            else:
                each(1, npair, lambda q: fn(kv_c(lax.rem(zh + q, npair), j)))

    ur = up_ref.shape[0] // 2

    def up_rows(p):
        return pl.ds(p * ur, ur)

    def up_part(j, p):
        return up_ref.at[up_rows(p), pl.ds(pl.multiple_of(j * fh, fh), fh)]

    def up_z(zz, p):
        return rc(up_part(zz % 2, p), up_buf.at[s, up_rows(p)], UP, rup.at[z * 2 + p], zz * 2 + y, t)

    def up_y0(p):
        return rc(up_part(zl, p), up_buf.at[s, up_rows(p)], UP, one.at[UP], y_sp, t)

    def up_fwd(zz, p):
        ref = up_buf.at[zz * 2 + y, up_rows(p)]
        arrived(ref, rup.at[zz * 2 + p])
        rc(ref, ref, UP, one.at[UP], y_sp, t).start()

    def cols_of(p):
        if pieces == 1:
            return pl.ds(0, pw)
        return pl.ds(p * pw if isinstance(p, int) else pl.multiple_of(p * pw, pw), pw)

    def dn_part(j, p):
        return dn_ref.at[dn_rows(j), cols_of(p)]

    def dn_z(zz, p):
        return rc(
            dn_part(zz % 2, p), dn_buf.at[s, :, cols_of(p)], DN, rdz.at[z * pieces + p], zz * 2 + y, t
        )

    def dn_y0(p):
        return rc(dn_part(zl, p), dn_buf.at[s, :, cols_of(p)], DN, rdy.at[z * pieces + p], y_sp, t)

    def dn_fwd(zz, p):
        ref = dn_buf.at[zz * 2 + y, :, cols_of(p)]
        arrived(ref, rdz.at[zz * pieces + p])
        rc(ref, ref, DN, rdy.at[zz * pieces + p], y_sp, t).start()

    def ow_x(k):
        return rc(ow_ref, ow_buf.at[t], OW, rox.at[k], s, lax.rem(x + k, nth) * 2 + c)

    def ow_s0():
        return rc(ow_ref, ow_buf.at[t], OW, one.at[OW], s, sib_t)

    def ow_fwd(k):
        ref = ow_buf.at[lax.rem(x + nth - k, nth) * 2 + c]
        arrived(ref, rox.at[k])
        rc(ref, ref, OW, one.at[OW], s, sib_t).start()

    def st_c(k):
        td = lax.rem(t + k, ntp)
        return rc(st_ref.at[rows_of(td), :], st_buf.at[t], ST, one.at[ST], s, td)

    def at_cols():
        return pl.ds(pl.multiple_of(y * vd, vd), vd)

    def at_c(i, tt):
        rows = pl.ds((i * ntp + tt) * share, share)
        return rc(
            at_snd.at[rows, :], at_buf.at[head_t, :, at_cols()], AT, one.at[AT], (zh * 2 + i) * 2 + c, tt
        )

    def at_all(fn):
        pl.when(y == c)(lambda: fn(at_snd.at[pl.ds(0, 2 * tok - share)]))
        pl.when(y != c)(lambda: fn(at_snd.at[pl.ds(0, 2 * tok)]))

    def grp_dev(g):
        return (zh * 2 + g // nth) * 2 + y, lax.rem(g, nth) * 2 + c

    def h_rows(g, n):
        return h_buf.at[c, g, pl.ds(n * (share // 2), share // 2), :]

    def own_rows(n):
        return h_own.at[pl.ds(n * (share // 2), share // 2), :]

    def h_z(n):
        return rc(own_rows(n), h_rows(grp, n), HP, rh.at[grp * 2 + n], mate * 2 + y, t)

    def h_x(k, n):
        dest = lax.rem(x + k, nth) * 2 + c
        return rc(own_rows(n), h_rows(grp, n), HP, rh.at[grp * 2 + n], s, dest)

    def h_s0(n):
        return rc(own_rows(n), h_rows(grp, n), HS, one.at[HS], s, sib_t)

    def h_fwd(zz, k, n, far=False):
        g = zz * nth + lax.rem(x + nth - k, nth)
        ref = h_rows(g, n)
        arrived(ref, rh.at[g * 2 + n])
        if far:
            for i in range(1, nth):
                rc(ref, ref, HP, rh.at[g * 2 + n], s, lax.rem(x + i, nth) * 2 + c).start()
        rc(ref, ref, HS, one.at[HS], s, sib_t).start()

    def sib_c(n):
        return rc(sib_snd.at[n], sib_buf.at[n], SIB, rsib.at[n], s, sib_t)

    def red_c(n, k):
        g = lax.rem(grp + k, ng)
        sp, tp = grp_dev(g)
        return rc(red_snd.at[n, g], red_buf.at[n, grp], RED, rred.at[n], sp, tp)

    def other(q, m):
        r = lax.rem(zh + q, npair)
        return r * 2 + jnp.where(r > zh, m, 1 - m)

    def shared(zz):
        return (zz > z) == (mate > z)

    inner = jnp.logical_not(shared(other(1, 0))) if npair > 1 else z < 0

    def others(fn):
        for m in range(2):
            each(1, npair, lambda q: fn(other(q, m)))

    barrier = pltpu.get_barrier_semaphore()

    def greet(sp, tp):
        pl.semaphore_signal(barrier, inc=1, device_id={"sp": sp, "tp": tp}, device_id_type=MESH)

    for o in range(4 * ntp):
        sp, tt = zh * 4 + o // ntp, o % ntp
        pl.when((sp != s) | (tt != t))(functools.partial(greet, sp, tt))

    def greet_far(q):
        for o in range(8):
            greet(lax.rem(zh + q, npair) * 4 + o // 2, x * 2 + o % 2)

    each(1, npair, greet_far)
    for ld in qk_loads + v_loads + [lam_load]:
        ld.start()

    for ld in qk_loads + [lam_load]:
        ld.wait()
    for j in range(heads):
        at = slice(j * qk, (j + 1) * qk)
        qsl[j] = jnp.concatenate([qin[0, :, at], qin[1, :, at]], axis=1)
        slab[j, :, :qw] = jnp.concatenate([kin[0, :, at], kin[1, :, at]], axis=1)
        lam_all[c, j] = jnp.full(lam_all.shape[2:], lam_in[0, j], F32)
    for ld in v_loads:
        ld.wait()
    pl.semaphore_wait(barrier, 4 * ntp - 1 + 8 * (npair - 1))

    for j in range(heads):
        pl.when(jnp.logical_not(to_self(j)))(lambda: q_c(j).start())
    kv_out(lambda cp: cp.start(), True)
    kv_out(lambda cp: cp.start(), False)
    for j in range(heads):
        @pl.when(to_self(j))
        def _():
            q_buf[zl] = qsl[j]
            kv_buf[s] = slab[j]

    lam_c().start()
    each(1, nth, lambda k: ow_x(k).start())
    each(1, ntp, lambda k: st_c(k).start())
    ow_s0().start()
    def up_far(p):
        each(1, npair, lambda q: up_z(other(q, 1), p).start())
        each(1, npair, lambda q: up_z(other(q, 0), p).start())

    for p in range(2):
        up_y0(p).start()
    for p in range(2):
        up_z(mate, p).start()
    up_far(0)
    for p in range(pieces):
        dn_y0(p).start()
    for ld in gain_loads + [st_load, ow_load, up_load, dn_load]:
        ld.start()

    m_run[...] = jnp.full(m_run.shape, -1e30, F32)
    l_run[...] = jnp.zeros(l_run.shape, F32)
    acc[...] = jnp.zeros(acc.shape, F32)
    scale = qk ** (-0.5)
    lane = lax.broadcasted_iota(jnp.int32, (tok, qw), 1)
    for i in range(2):
        pl.when(jnp.logical_not(self_worker & (zl == i)))(lambda: arrived(q_buf.at[i], rq.at[i]))
        qv = q_buf[i].astype(F32) * scale
        for mp in range(2):
            keep = (lane >= mp * qk) & (lane < (mp + 1) * qk)
            qm[mp, i * tok : (i + 1) * tok, :] = jnp.where(keep, qv, 0.0).astype(BF16)

    pl.when(inner)(lambda: up_far(1))

    def absorb(block):
        v = block[:, qw:]
        for r in range(2):
            sc = lax.dot_general(block[:, :qw], qm[r], NT, preferred_element_type=F32)
            old = m_run[r]
            new = jnp.maximum(old, jnp.max(sc, axis=0, keepdims=True))
            fac = jnp.exp(old - new)
            ex = jnp.exp(sc - new)
            l_run[r] = l_run[r] * fac + jnp.sum(ex, axis=0, keepdims=True)
            acc[r] = acc[r] * fac + lax.dot_general(
                v, ex.astype(BF16), TN, preferred_element_type=F32
            )
            m_run[r] = new

    def step(i, carry):
        zz = lax.rem(zh * 2 + i // 2, nz)
        own = lax.rem(i, 2) == 0

        @pl.when(own)
        def _():
            direct = kv_buf.at[zz * 2 + c]
            pl.when(jnp.logical_not(self_worker & (zz == z)))(lambda: arrived(direct, rkv.at[zz]))
            kv_s(zz).start()

        pl.when(jnp.logical_not(own))(lambda: arrived(kv_buf.at[zz * 2 + 1 - c], rkvs.at[zz]))
        absorb(kv_buf.at[zz * 2 + jnp.where(own, c, 1 - c)])
        return carry

    lax.fori_loop(0, nsp, step, 0)

    for ld in gain_loads:
        ld.wait()
    arrived(lam_all.at[c], one.at[LAM])
    lam = lam_all[zl, y][:, :1]
    mixed = acc[0] / l_run[0] - lam * (acc[1] / l_run[1])
    inv = lax.rsqrt(jnp.mean(jnp.square(mixed), axis=0, keepdims=True) + 1e-05)
    normed = jnp.transpose(mixed * inv) * hg[...] * 0.8
    at_snd[...] = normed.astype(BF16)
    spots = [(i, tt) for i in range(2) for tt in range(ntp)]

    def at_mine(i, tt):
        return (i == zl) & (y == c) & (tt == t)

    for i, tt in spots:
        pl.when(jnp.logical_not(at_mine(i, tt)))(lambda: at_c(i, tt).start())

        @pl.when(at_mine(i, tt))
        def _():
            n = (i * ntp + tt) * share
            at_buf[head_t, :, at_cols()] = at_snd[n : n + share, :]

    def others_fwd(p):
        each(1, npair, lambda q: [up_fwd(other(q, m), p) for m in range(2)])

    pl.when(jnp.logical_not(inner))(lambda: up_far(1))
    for p in range(2):
        up_fwd(mate, p)
    for k in range(1, nth):
        ow_fwd(k)
    others_fwd(0)
    st_load.wait()
    arrived(st_buf.at[pl.ds(0, ntp - 1)], one.at[ST])
    cols = st_ref.shape[1]
    for b in range(ntp):
        pre[:, b * cols : (b + 1) * cols] = ALPHA * st_buf[b].astype(F32)
    at_all(lambda ref: arrived(ref, one.at[AT]))
    ow_load.wait()
    arrived(ow_buf.at[pl.ds(0, nth)], one.at[OW])
    for b in range(ntp):
        at = slice(b * cols, (b + 1) * cols)
        tot = pre[:, at]
        for tt in range(ntp):
            tot += jnp.dot(at_buf[tt], ow_buf[tt, :, at], preferred_element_type=F32)
        pre[:, at] = tot
    h_own[...] = layer_norm(pre[...], g1[...]).astype(BF16)
    for n in range(2):
        h_z(n).start()
        for k in range(1, nth):
            h_x(k, n).start()
        h_s0(n).start()
    for p in range(pieces):
        dn_z(mate, p).start()
    for p in range(pieces):
        each(1, npair, lambda q: dn_z(other(q, 0), p).start())
    h_buf[c, grp] = h_own[...]
    others_fwd(1)

    for n in range(2):
        h_fwd(1 - zl, 0, n, True)
    for p in range(pieces):
        each(1, npair, lambda q: dn_z(other(q, 1), p).start())
    for zz in (zl, 1 - zl):
        for n in range(2):
            for k in range(1, nth):
                h_fwd(zz, k, n)
    up_load.wait()
    arrived(up_buf.at[pl.ds(0, nz)], one.at[UP])
    arrived(h_buf.at[0], one.at[HS])

    half = ng * share
    for side in range(2):
        parts = 2 if fh % 256 == 0 else 1
        for n in range(parts):
            wide = fh // parts
            at = slice(n * wide, (n + 1) * wide)
            hid = h_buf[side].reshape(half, d)
            w = up_buf[:, :, at].reshape(d, wide)
            up = jnp.dot(hid, w, preferred_element_type=F32)
            act[side, :, at] = jnp.square(jnp.maximum(up, 0.0)).astype(BF16)
    dn_load.wait()

    steps = nz * pieces

    def unit(i):
        r = lax.rem(i, 2 * pieces)
        far = other(i // (2 * pieces), lax.rem(r, 2))
        zz = jnp.where(i < pieces, z, jnp.where(i < 2 * pieces, mate, far))
        return zz, jnp.where(i < 2 * pieces, lax.rem(i, pieces), r // 2)

    def index(i):
        zz, p = unit(i)
        return zz * pieces + p

    def finish(n):
        arrived(sib_buf.at[n], rsib.at[n])
        for k in range(1, ng):
            g = lax.rem(grp + k, ng)
            rows = pl.ds(pl.multiple_of(g * share, share), share)
            red_snd[n, g] = (part[n, :, rows, :] + sib_buf[n, :, rows, :].astype(F32)).astype(BF16)
            red_c(n, k).start()
        rows = pl.ds(pl.multiple_of(grp * share, share), share)
        own_part[n] = part[n, :, rows, :] + sib_buf[n, :, rows, :].astype(F32)

    ahead, lead = pieces, 2

    def down(i, carry):
        pl.when((i + lead >= ahead) & (i + lead < steps))(lambda: dn_fwd(*unit(i + lead)))
        pl.when(i > 0)(lambda: finish(index(i - 1)))
        zz, p = unit(i)
        n = zz * pieces + p
        arrived(dn_buf.at[zz * 2 + 1 - y, :, cols_of(p)], rdy.at[n])
        at = cols_of(p)
        for yy in range(2):
            res = jnp.dot(act[1 - c], dn_buf[zz * 2 + yy, :, at], preferred_element_type=F32)
            sib_snd[n, yy] = res.astype(BF16)
        sib_c(n).start()
        for yy in range(2):
            part[n, yy] = jnp.dot(act[c], dn_buf[zz * 2 + yy, :, at], preferred_element_type=F32)
        return carry

    lax.fori_loop(0, steps, down, 0)
    finish(index(steps - 1))

    for zz in range(nz):
        for p in range(pieces):
            n = zz * pieces + p
            arrived(red_buf.at[n, pl.ds(0, ng - 1)], rred.at[n])
            for yy in range(2):
                lo = (zz * 2 + yy) * out_w + p * pw
                at = slice(lo, lo + pw)
                tot = own_part[n, yy] + ALPHA * h_own[:, at].astype(F32)
                for k in range(ng - 1, 0, -1):
                    tot += red_buf[n, lax.rem(grp + ng - k, ng), yy].astype(F32)
                pre[:, at] = tot
    out_ref[...] = layer_norm(pre[...], g2[...]).astype(BF16)

    for kind, buf, most in ((Q, qsl, heads), (KV, kv_buf, npair * heads)):
        pl.when(self_worker)(lambda: left(buf.at[pl.ds(0, most - 1)], kind))
        pl.when(jnp.logical_not(self_worker))(lambda: left(buf.at[pl.ds(0, most)], kind))
    at_all(lambda ref: left(ref, AT))
    left(lam_all.at[c], LAM)
    left(kv_buf.at[pl.ds(0, nz)], KVS)
    left(up_buf.at[pl.ds(0, nsp - 1)], UP)
    left(dn_buf.at[pl.ds(0, nsp - 1)], DN)
    left(ow_buf.at[pl.ds(0, ntp - 1)], OW)
    left(st_buf.at[pl.ds(0, ntp - 1)], ST)
    left(h_buf.at[0, pl.ds(0, ng - 1)], HP)
    left(h_buf.at[0], HS)
    left(sib_snd, SIB)
    left(red_snd.at[:, pl.ds(0, ng - 1)], RED)


def local(nsp, ntp, q1, q2, k1, k2, vals, lam, hg, stream, ow, g1, up, dn, g2):
    tok = q1.shape[0]
    heads = lam.shape[0]
    hv = vals.shape[1]
    vd = hv // heads
    d = ow.shape[1]
    nz, nth = nsp // 2, ntp // 2
    ng = 2 * nth
    share = tok // ntp
    fh = up.shape[1] // 2
    qk = q1.shape[1] // heads
    half, out_w = ng * share, dn.shape[1]
    pieces = 2 if out_w % 256 == 0 else 1
    units, pw = nz * pieces, out_w // pieces
    vm = pl.BlockSpec(memory_space=pltpu.VMEM)
    hbm = pl.BlockSpec(memory_space=pl.ANY)
    sems = (KINDS, KINDS, 2, nz, nz, 2 * nz, units, units, nth, 2 * ng, units, units)
    return pl.pallas_call(
        functools.partial(kernel, nsp, ntp, heads, pieces),
        out_shape=pltpu.VMEM((share, d), BF16),
        in_specs=[hbm] * 13,
        out_specs=vm,
        scratch_shapes=[
            pltpu.SMEM((1, heads), F32),
            pltpu.VMEM((2, heads, 1, 128), F32),
            pltpu.VMEM((2, tok, heads * qk), BF16),
            pltpu.VMEM((2, tok, heads * qk), BF16),
            pltpu.VMEM((heads, tok, 2 * qk), BF16),
            pltpu.VMEM((heads, tok, 2 * qk + vd), BF16),
            pltpu.VMEM((1, vd), F32),
            pltpu.VMEM((1, d), F32),
            pltpu.VMEM((1, d), F32),
            pltpu.VMEM((2, tok, 2 * qk), BF16),
            pltpu.VMEM((2, 2 * tok, 2 * qk), BF16),
            pltpu.VMEM((2, 1, 2 * tok), F32),
            pltpu.VMEM((2, 1, 2 * tok), F32),
            pltpu.VMEM((2, vd, 2 * tok), F32),
            pltpu.VMEM((nsp, tok, 2 * qk + vd), BF16),
            pltpu.VMEM((nsp, up.shape[0], fh), BF16),
            pltpu.VMEM((nsp, fh, out_w), BF16),
            pltpu.VMEM((ntp,) + ow.shape, BF16),
            pltpu.VMEM((ntp, share, stream.shape[1]), BF16),
            pltpu.VMEM((2 * tok, vd), BF16),
            pltpu.VMEM((ntp, share, hv), BF16),
            pltpu.VMEM((share, d), F32),
            pltpu.VMEM((share, d), BF16),
            pltpu.VMEM((2, ng, share, d), BF16),
            pltpu.VMEM((2, half, fh), BF16),
            pltpu.VMEM((units, 2, half, pw), BF16),
            pltpu.VMEM((units, 2, half, pw), BF16),
            pltpu.VMEM((units, 2, half, pw), F32),
            pltpu.VMEM((units, 2, share, pw), F32),
            pltpu.VMEM((units, ng, 2, share, pw), BF16),
            pltpu.VMEM((units, ng, 2, share, pw), BF16),
            pltpu.SemaphoreType.DMA((5 + heads + 7,)),
            *[pltpu.SemaphoreType.DMA((n,)) for n in sems],
        ],
        compiler_params=pltpu.CompilerParams(
            collective_id=0, has_side_effects=True, vmem_limit_bytes=60 * 1024 * 1024
        ),
    )(
        lam.reshape(1, heads), q1, q2, k1, k2, vals, hg.reshape(1, vd), stream, ow,
        g1.reshape(1, d), up, dn, g2.reshape(1, d),
    )


def solution(mesh):
    in_specs = (
        P("sp", "tp"),
        P("sp", "tp"),
        P("sp", "tp"),
        P("sp", "tp"),
        P("sp", "tp"),
        P("tp"),
        P(),
        P("sp", "tp"),
        P("tp", None),
        P(),
        P("sp", "tp"),
        P("tp", "sp"),
        P(),
    )
    body = functools.partial(local, mesh.shape["sp"], mesh.shape["tp"])
    return jax.shard_map(
        body, mesh=mesh, in_specs=in_specs, out_specs=P(("sp", "tp"), None), check_vma=False
    )
```
